32 devices in a mesh: rep: 2 (over x), fs: 8 (over z, y), tp: 2 (over core).
Axes of the slice: x: 2, y: 2, z: 4, core: 2. Of those that a mesh axis runs over, the one named last changes fastest.
Arguments:
- x_late: bfloat16 [2048, 2048], P(('rep', 'fs')), parts along dimension 0, may hold values from -6 to 6
- x_early: bfloat16 [2048, 2048], P(('rep', 'fs')), parts along dimension 0, may hold values from -6 to 6
- cotangent: bfloat16 [2048, 2048], P(('rep', 'fs')), parts along dimension 0, may hold values from -6 to 6
- pre_gain: float32 [2048], replicated, may hold values from 0.1 to 1.9
- post_gain: float32 [2048], replicated, may hold values from 0.1 to 1.9
- gate_weight: bfloat16 [2048, 3072], P('fs', 'tp'), may hold values from -0.125 to 0.125
- up_weight: bfloat16 [2048, 3072], P('fs', 'tp'), may hold values from -0.125 to 0.125
- down_weight: bfloat16 [2048, 3072], P('fs', 'tp'), may hold values from -0.109375 to 0.109375
- down_grad_sum: float32 [4096, 3072], P(('rep', 'fs'), 'tp'), parts along dimension 0, may hold values from -6 to 6
Outputs:
- y_late: bfloat16 [2048, 2048], P(('rep', 'fs')), parts along dimension 0
- dx_early: bfloat16 [2048, 2048], P(('rep', 'fs')), parts along dimension 0
- down_grad_out: float32 [4096, 3072], P(('rep', 'fs'), 'tp'), parts along dimension 0
The draws below stay inside these ranges and needn't reach their ends.
There are 2 independent parts, one for each index of `rep`. The reference program is written for one: setup_inputs(seed, part) draws one part's arguments, and reference() takes and returns one part's arrays. A program takes and returns all parts, laid end to end along the dimension named above; an argument that names none is the same for every part. Nothing has to cross between parts.
All inputs are finite; a program needn't handle non-finite values.
Results may differ from the reference program's by a relative error of at most 0.023.
Values may be sent and summed in bfloat16 or wider, within the bound.
No kernel may reach another device: no remote copies, remote signals or barrier semaphores. Data moves between devices by JAX's collectives and lax.ppermute only.
A program may use at most 64 MiB of HBM per device.

```python
import jax
import jax.numpy as jnp
from jax import lax

D = 2048
FF = 3072
TOKENS = 1024
N_TP = 2


def strengthened(array, key, source, target, blocks, factor):
    owner, partner = [(jnp.arange(array.shape[position]) // (array.shape[position] // blocks)).reshape([-1 if axis == position else 1 for axis in range(array.ndim)]) for position in (source, target)]
    chosen = jax.random.permutation(key, blocks)[partner]
    strong = (owner == chosen) | (owner == (partner + blocks // 2) % blocks)
    return jnp.where(strong, factor * array, array)


def block_scale(own_key, dims, pieces, smallest, top_value):
    def one(position, parts):
        heights = jax.random.uniform(jax.random.fold_in(jax.random.fold_in(own_key, 6), position), (parts,), jnp.float32, smallest / len(pieces), top_value / len(pieces))
        return jnp.repeat(jnp.exp(heights), dims[position] // parts).reshape((-1,) + (1,) * (len(dims) - position - 1))

    level = one(*pieces[0])
    for cut in pieces[1:]:
        level = level * one(*cut)
    return level


def noise(key, dims, scale, most, shards=(), dtype=jnp.bfloat16):
    loudness = block_scale(key, dims, shards, -0.22, 0.18) if shards else 1.0
    result = jax.random.normal(key, dims, jnp.float32) * scale * loudness
    return jnp.minimum(jnp.maximum(result, -most), most).astype(dtype)


def gaussian_with(rng, dims, spread, most, pieces, heavy, held_as=jnp.bfloat16):
    result = spread * jax.random.normal(rng, dims, jnp.float32)
    if pieces:
        result = result * block_scale(rng, dims, pieces, -0.22, 0.18)
    return jnp.clip(strengthened(result, jax.random.fold_in(rng, 3), *heavy), -most, most).astype(held_as)


def setup_inputs(seed: int = 0, part: int = 0) -> dict:
    splits = jax.random.split(jax.random.key(seed), 10)
    part_keys = jax.random.split(jax.random.fold_in(splits[9], part), 10)
    return {
        "x_late": noise(part_keys[0], (TOKENS, D), 1.0, 6.0, ((0, 8),)),
        "x_early": noise(part_keys[1], (TOKENS, D), 1.0, 6.0, ((0, 8),)),
        "cotangent": gaussian_with(part_keys[2], (TOKENS, D), 1.0, 6.0, ((0, 8),), (0, 1, 8, 2.0)),
        "pre_gain": jnp.clip(1.0 + 0.18 * jax.random.normal(splits[3], (D,), jnp.float32), 0.1, 1.9),
        "post_gain": jnp.clip(1.0 + 0.18 * jax.random.normal(splits[4], (D,), jnp.float32), 0.1, 1.9),
        "gate_weight": noise(splits[5], (D, FF), D ** -0.5, 0.125, ((0, 8), (1, 2))),
        "up_weight": noise(splits[6], (D, FF), D ** -0.5, 0.125, ((0, 8), (1, 2))),
        "down_weight": noise(splits[7], (D, FF), FF ** -0.5, 0.109375, ((0, 8), (1, 2))),
        "down_grad_sum": noise(part_keys[8], (D, FF), 1.0, 6.0, ((0, 8), (1, 2)), jnp.float32),
    }


eps = 1e-06

def pre_norm(x, pre_gain):
    xf = x.astype(jnp.float32)
    scale = lax.rsqrt(lax.optimization_barrier(jnp.mean(xf * xf, axis=-1, keepdims=True)) + eps)
    return (xf, scale, (xf * scale * pre_gain).astype(jnp.bfloat16))

def block_sum(left, right, width):
    total = jnp.zeros((left.shape[0], right.shape[0]), jnp.float32)
    for block in range(N_TP):
        lo = block * width
        term = lax.dot_general(left[:, lo:lo + width], right[:, lo:lo + width], (((1,), (1,)), ((), ())), preferred_element_type=jnp.float32)
        term = lax.optimization_barrier(term.astype(jnp.bfloat16))
        total = total + term.astype(jnp.float32)
    return total

def forward_branch(normed, gate_weight, up_weight, down_weight):
    gate = jnp.dot(normed, gate_weight, preferred_element_type=jnp.float32)
    up = jnp.dot(normed, up_weight, preferred_element_type=jnp.float32)
    hidden = (jax.nn.silu(gate) * up).astype(jnp.bfloat16)
    branch = block_sum(hidden, down_weight, FF // N_TP)
    return (gate, up, hidden, branch)

def reference(x_late, x_early, cotangent, pre_gain, post_gain, gate_weight, up_weight, down_weight, down_grad_sum):
    width = FF // N_TP
    late_f, late_rs, late_norm = pre_norm(x_late, pre_gain)
    gate_l, up_l, hidden_l, branch_l = forward_branch(late_norm, gate_weight, up_weight, down_weight)
    late_rz = lax.rsqrt(lax.optimization_barrier(jnp.mean(branch_l * branch_l, axis=-1, keepdims=True)) + eps)
    y_late = (late_f + 0.5 * branch_l * late_rz * post_gain).astype(jnp.bfloat16)
    early_f, early_rs, early_norm = pre_norm(x_early, pre_gain)
    gate_e, up_e, hidden_e, branch_e = forward_branch(early_norm, gate_weight, up_weight, down_weight)
    early_rz = lax.rsqrt(lax.optimization_barrier(jnp.mean(branch_e * branch_e, axis=-1, keepdims=True)) + eps)
    cot_f = cotangent.astype(jnp.float32)
    dpost = 0.5 * cot_f * post_gain
    dbranch = early_rz * (dpost - branch_e * early_rz * early_rz * lax.optimization_barrier(jnp.mean(branch_e * dpost, axis=-1, keepdims=True)))
    dbranch = dbranch.astype(jnp.bfloat16)
    dhidden = jnp.dot(dbranch, down_weight, preferred_element_type=jnp.float32)
    sig = jax.nn.sigmoid(gate_e)
    dgate = (dhidden * up_e * sig * (1.0 + gate_e * (1.0 - sig))).astype(jnp.bfloat16)
    dup = (dhidden * gate_e * sig).astype(jnp.bfloat16)
    dnormed = jnp.zeros(x_early.shape, jnp.float32)
    for block in range(N_TP):
        lo = block * width
        term = lax.dot_general(dgate[:, lo:lo + width], gate_weight[:, lo:lo + width], (((1,), (1,)), ((), ())), preferred_element_type=jnp.float32)
        term = term + lax.dot_general(dup[:, lo:lo + width], up_weight[:, lo:lo + width], (((1,), (1,)), ((), ())), preferred_element_type=jnp.float32)
        term = lax.optimization_barrier(term.astype(jnp.bfloat16))
        dnormed = dnormed + term.astype(jnp.float32)
    gained = pre_gain * dnormed
    dx_early = cot_f + early_rs * (gained - early_f * early_rs * early_rs * lax.optimization_barrier(jnp.mean(early_f * gained, axis=-1, keepdims=True)))
    dx_early = dx_early.astype(jnp.bfloat16)
    down_grad_out = down_grad_sum + lax.dot_general(dbranch, hidden_e, (((0,), (0,)), ((), ())), preferred_element_type=jnp.float32)
    return (y_late, dx_early, down_grad_out)
```

```python
import jax
import jax.numpy as jnp
from jax import lax
from jax.sharding import PartitionSpec as P

eps = 1e-06
AXES = ("rep", "fs", "tp")
f32 = jnp.float32
bf16 = jnp.bfloat16


def nt(left, right):
    return lax.dot_general(left, right, (((1,), (1,)), ((), ())), preferred_element_type=f32)


def tn(left, right):
    return lax.dot_general(left, right, (((0,), (0,)), ((), ())), preferred_element_type=f32)


def pick(array, index):
    return lax.dynamic_index_in_dim(array, index, 0, keepdims=False)


def put(array, value, index):
    return lax.dynamic_update_index_in_dim(array, value, index, 0)


def make_body(R, S, T):
    G = 2 if S % 2 == 0 else 1
    Z = S // G
    peers = [(a, b) for a in range(R) for b in range(G)]
    others = peers[1:]

    def send(value, dr=0, dy=0, dz=0, dt=0, lo=0, hi=None, wrap=False):
        hi = Z - 1 if hi is None else hi
        pairs = []
        for r in range(R):
            for z in range(Z):
                for y in range(G):
                    for t in range(T):
                        to = z + dz
                        if wrap:
                            to %= Z
                        if not (lo <= z <= hi and 0 <= to < Z):
                            continue
                        source = (r * S + z * G + y) * T + t
                        target = ((r + dr) % R * S + to * G + (y + dy) % G) * T + (t + dt) % T
                        pairs.append((source, target))
        return lax.ppermute(value, AXES, pairs)

    def line(piece):
        up, down, below, above = piece, piece, [], []
        for s in range(1, Z):
            up = send(up, dz=1, lo=s - 1)
            down = send(down, dz=-1, hi=Z - s)
            below.append(up)
            above.append(down)
        return below, above

    def order(z):
        hops = range(1, Z)
        table = []
        for s in hops:
            if z >= s:
                table.append((0, s))
            if z + s < Z:
                table.append((1, s))
        return table

    def body(x_late, x_early, cotangent, pre_gain, post_gain, gate_weight, up_weight, down_weight, down_grad_sum):
        r, f, t = (lax.axis_index(a) for a in AXES)
        y, z = f % G, f // G
        n, D = x_late.shape
        m = n // T
        K, F = gate_weight.shape
        w = F // (R * G)
        PT = len(peers)

        def columns(weight, dy):
            q = r * G + (y + dy) % G
            return lax.dynamic_slice_in_dim(weight, q * w, w, 1)

        def both(dy):
            return jnp.concatenate([columns(gate_weight, dy), columns(up_weight, dy)], axis=1)

        gu = [both(0)] + [send(both(d), dy=d) for d in range(1, G)]
        dn = [columns(down_weight, 0)] + [send(columns(down_weight, d), dy=d) for d in range(1, G)]

        x = jnp.stack([x_late, x_early]).astype(f32)
        scale = lax.rsqrt(jnp.mean(x * x, axis=-1, keepdims=True) + eps)
        normed = (x * scale * pre_gain).astype(bf16).reshape(2, T, m, D)

        def chunk(array, j):
            return lax.dynamic_index_in_dim(array, (t + j) % T, 1, keepdims=False)

        mine = chunk(normed, 0)
        held = [[chunk(normed, j) for j in range(T)]]
        for dr, dy in others:
            got = send(mine, dr=-dr, dy=-dy)
            held.append([got] + [send(got, dt=-j) for j in range(1, T)])
        tokens = jnp.stack([jnp.stack(h, axis=1) for h in held], axis=1).reshape(2 * PT * n, D)

        full = jnp.zeros((Z, G, K, 2 * w), bf16)

        def place(array, value, zi, yi):
            return lax.dynamic_update_slice(array, value[None, None], (zi, yi, 0, 0))

        lines = [line(piece) for piece in gu]
        for s in range(1, Z):
            for d, (below, above) in enumerate(lines):
                yi = (y - d) % G
                full = place(full, below[s - 1], jnp.where(z >= s, z - s, z), yi)
                full = place(full, above[s - 1], jnp.where(z + s < Z, z + s, z), yi)
        for d, piece in enumerate(gu):
            full = place(full, piece, z, (y - d) % G)
        full = full.reshape(D, 2 * w)

        both_out = jnp.dot(tokens, full, preferred_element_type=f32)
        gate, up = both_out[:, :w], both_out[:, w:]
        hidden = (jax.nn.silu(gate) * up).astype(bf16)

        block = jnp.zeros((G, K, w), bf16)
        for d, piece in enumerate(dn):
            block = put(block, piece, (y - d) % G)
        block = block.reshape(G * K, w)
        below, above = line(block)
        got = (below, above)
        slots, ids = [block], [z]
        tables = [order(i) for i in range(Z)]
        for k in range(Z - 1):
            value, where = None, jnp.int32(0)
            for side, s in sorted({tables[i][k] for i in range(Z)}):
                owners = [i for i in range(Z) if tables[i][k] == (side, s)]
                here = sum((z == i) for i in owners).astype(bool)
                value = got[side][s - 1] if value is None else jnp.where(here, got[side][s - 1], value)
                where = jnp.where(here, z + (s if side else -s), where)
            slots.append(value)
            ids.append(where)

        def reduce_plane(part):
            low = part.astype(bf16)
            chip = part[:, :, 0]
            for j in range(1, T):
                chip = chip + send(low[:, :, j], dt=j).astype(f32)
            low = chip.astype(bf16)
            total = chip[:, 0]
            for p, (dr, dy) in enumerate(peers):
                if p:
                    total = total + send(low[:, p], dr=dr, dy=dy).astype(f32)
            return total

        groups = [[0, 1]] + [[k] for k in range(2, Z)] if Z > 1 else [[0]]
        branch = jnp.zeros((Z, 2, m, G * K), f32)
        for group in groups:
            weight = jnp.concatenate([slots[k] for k in group], axis=0)
            part = nt(hidden, weight).reshape(2, PT, T, m, len(group) * G * K)
            total = reduce_plane(part)
            for i, k in enumerate(group):
                branch = put(branch, total[:, :, i * G * K:(i + 1) * G * K], ids[k])
        branch = branch.transpose(1, 2, 0, 3).reshape(2, m, D)
        branch_l, branch_e = branch[0], branch[1]

        def own_rows(array):
            return lax.dynamic_slice_in_dim(array, t * m, m, 0)

        def all_rows(value):
            out = put(jnp.zeros((T,) + value.shape, value.dtype), value, t)
            for j in range(1, T):
                out = put(out, send(value, dt=-j), (t + j) % T)
            return out.reshape(n, D)

        late_rz = lax.rsqrt(jnp.mean(branch_l * branch_l, axis=-1, keepdims=True) + eps)
        y_late = (own_rows(x_late).astype(f32) + 0.5 * branch_l * late_rz * post_gain).astype(bf16)
        y_late = all_rows(y_late)

        early_rz = lax.rsqrt(jnp.mean(branch_e * branch_e, axis=-1, keepdims=True) + eps)
        cot_f = own_rows(cotangent).astype(f32)
        dpost = 0.5 * cot_f * post_gain
        dbranch = early_rz * (dpost - branch_e * early_rz * early_rz * jnp.mean(branch_e * dpost, axis=-1, keepdims=True))
        dbranch = dbranch.astype(bf16)

        def plane(value):
            out = []
            for p, (dr, dy) in enumerate(peers):
                got = send(value, dr=-dr, dy=-dy) if p else value
                out.append([got] + [send(got, dt=-j) for j in range(1, T)])
            return out

        down_full = jnp.zeros((Z, G * K, w), bf16)
        for slot, where in zip(slots, ids):
            down_full = put(down_full, slot, where)
        down_full = down_full.reshape(D, w)
        spread = plane(dbranch)
        spread = jnp.stack([jnp.stack(h) for h in spread]).reshape(PT * n, D)
        dhidden = jnp.dot(spread, down_full, preferred_element_type=f32)
        gate_e, up_e = gate[PT * n:], up[PT * n:]
        sig = jax.nn.sigmoid(gate_e)
        dgate = (dhidden * up_e * sig * (1.0 + gate_e * (1.0 - sig))).astype(bf16)
        dup = (dhidden * gate_e * sig).astype(bf16)
        dpart = nt(jnp.concatenate([dgate, dup], axis=1), full)
        dnormed = reduce_plane(dpart.reshape(1, PT, T, m, D))[0]
        gained = pre_gain * dnormed
        early_f = own_rows(x_early).astype(f32)
        early_rs = lax.dynamic_slice_in_dim(scale[1], t * m, m, 0)
        dx = cot_f + early_rs * (gained - early_f * early_rs * early_rs * jnp.mean(early_f * gained, axis=-1, keepdims=True))
        dx_early = all_rows(dx.astype(bf16))

        hidden_e = hidden[PT * n:]
        kept = [hidden_e] + [send(hidden_e, dz=k, wrap=True) for k in range(1, Z)]
        parts = dbranch.reshape(m, Z, G * K).transpose(1, 0, 2)
        cols = [pick(parts, z)] + [send(pick(parts, (z + k) % Z), dz=k, wrap=True) for k in range(1, Z)]
        wide = plane(jnp.stack(cols))
        half = G * n
        result = jnp.zeros((R * G, K, w), f32)
        for a in range(R):
            left = jnp.concatenate([wide[a * G + b][j][k] for k in range(Z) for b in range(G) for j in range(T)], axis=0)
            right = jnp.concatenate([h[a * half:(a + 1) * half] for h in kept], axis=0)
            grad = tn(left, right).reshape(G, K, w)
            for b in range(G):
                piece = pick(grad, (y + b) % G)
                if a or b:
                    piece = send(piece.astype(bf16), dr=a, dy=b).astype(f32)
                result = put(result, piece, (r - a) % R * G + (y - b) % G)
        summed = result.transpose(1, 0, 2).reshape(K, F)
        return (y_late, dx_early, down_grad_sum + summed)

    return body


def solution(mesh):
    R, S, T = (mesh.shape[a] for a in AXES)
    in_specs = (
        P(("rep", "fs"), None),
        P(("rep", "fs"), None),
        P(("rep", "fs"), None),
        P(),
        P(),
        P("fs", "tp"),
        P("fs", "tp"),
        P("fs", "tp"),
        P(("rep", "fs"), "tp"),
    )
    out_specs = (P(("rep", "fs"), None), P(("rep", "fs"), None), P(("rep", "fs"), "tp"))
    return jax.shard_map(make_body(R, S, T), mesh=mesh, in_specs=in_specs, out_specs=out_specs, check_vma=False)
```

```python
import jax
import jax.numpy as jnp
from jax import lax
from jax.experimental import pallas as pl
from jax.experimental.pallas import tpu as pltpu
from jax.sharding import PartitionSpec as P


eps = 1e-06
AXES = ("rep", "fs", "tp")
f32 = jnp.float32
bf16 = jnp.bfloat16


def nt(left, right):
    return lax.dot_general(left, right, (((1,), (1,)), ((), ())), preferred_element_type=f32)


def tn(left, right):
    return lax.dot_general(left, right, (((0,), (0,)), ((), ())), preferred_element_type=f32)


def pick(array, index):
    return lax.dynamic_index_in_dim(array, index, 0, keepdims=False)


def put(array, value, index):
    return lax.dynamic_update_index_in_dim(array, value, index, 0)


def arrange(values, ids, count, axis=-1):
    out = []
    for i in range(count):
        value = values[0]
        for k in range(1, len(values)):
            value = jnp.where(ids[k] == i, values[k], value)
        out.append(value)
    return jnp.concatenate(out, axis=axis)


def after(value, *others):
    return lax.optimization_barrier((value,) + others)[0]


def whole(n, scalar=0):
    vmem = [pl.BlockSpec(memory_space=pltpu.VMEM)] * n
    return [pl.BlockSpec(memory_space=pltpu.SMEM)] * scalar + vmem


def here(z, owners):
    hit = z == owners[0]
    for i in owners[1:]:
        hit = hit | (z == i)
    return hit


def by_slot(zref, slots, refs, count, emit):
    at = 0
    for k, slot in enumerate(slots):
        for owners in slot:
            ref = refs[at]
            at += 1
            if len(owners) == count:
                emit(k, ref)
            else:
                pl.when(here(zref[0], owners))(lambda k=k, ref=ref: emit(k, ref))


def sent_product(z, left, slots, count):
    rows, (columns, w) = left.shape[0], slots[0][0][0].shape
    owners = [[o for _, o in slot] for slot in slots]
    values = [v for slot in slots for v, _ in slot]

    def kernel(zref, left_ref, *refs):
        out = refs[-1]

        def emit(k, ref):
            out[:, k * columns:(k + 1) * columns] = nt(left_ref[...], ref[...]).astype(bf16)

        by_slot(zref, owners, refs, count, emit)

    return pl.pallas_call(
        kernel,
        out_shape=jax.ShapeDtypeStruct((rows, len(slots) * columns), bf16),
        in_specs=whole(1 + len(values), 1),
        out_specs=whole(1)[0],
        cost_estimate=pl.CostEstimate(flops=2 * rows * w * columns * len(slots), bytes_accessed=4 * rows * columns, transcendentals=0),
    )(z, left, *values)


def chip_product(z, left, got, slots, count, lead, parts):
    rows, (columns, w) = left.shape[0], slots[0][0][0].shape
    m = rows // (lead * parts)
    owners = [[o for _, o in slot] for slot in slots]
    values = [v for slot in slots for v, _ in slot]

    def kernel(zref, left_ref, *refs):
        received, refs, outs = refs[:len(got)], refs[len(got):-parts], refs[-parts:]

        def emit(k, ref):
            span = slice(k * columns, (k + 1) * columns)
            chip = nt(left_ref[...], ref[...])
            for other in received:
                chip = chip + other[:, span].astype(f32)
            chip = chip.astype(bf16)
            for a in range(lead):
                for p, out in enumerate(outs):
                    out[a * m:(a + 1) * m, span] = chip[(a * parts + p) * m:(a * parts + p + 1) * m]

        by_slot(zref, owners, refs, count, emit)

    return pl.pallas_call(
        kernel,
        out_shape=[jax.ShapeDtypeStruct((lead * m, len(slots) * columns), bf16)] * parts,
        in_specs=whole(1 + len(got) + len(values), 1),
        out_specs=whole(parts),
        cost_estimate=pl.CostEstimate(flops=2 * rows * w * columns * len(slots), bytes_accessed=8 * rows * columns, transcendentals=0),
    )(z, left, *got, *values)


def plan(R, S):
    G = 2 if S % 2 == 0 else 1
    Z = S // G
    peers = [(a, b) for a in range(R) for b in range(G)]
    ways = sorted(range(1, len(peers)), key=lambda p: (peers[p][0] == 0, peers[p][1] != 0))
    return G, Z, peers, ways


def edges(Z, s):
    out = []
    for kind in (0, 1):
        pairs = []
        for i in range(kind, Z - 1, 2):
            if i - (s - 1) >= 0:
                pairs.append((i, i + 1))
            if i + s < Z:
                pairs.append((i + 1, i))
        if pairs:
            out.append((kind, pairs))
    return out


def make_body(R, S, T):
    G, Z, peers, ways = plan(R, S)

    def send(value, dr=0, dy=0, dz=0, dt=0, moves=None):
        moves = [(z, (z + dz) % Z) for z in range(Z)] if moves is None else moves
        pairs = []
        for r in range(R):
            for z, to in moves:
                for y in range(G):
                    for t in range(T):
                        source = (r * S + z * G + y) * T + t
                        target = ((r + dr) % R * S + to * G + (y + dy) % G) * T + (t + dt) % T
                        pairs.append((source, target))
        return lax.ppermute(value, AXES, pairs)

    def line(piece):
        got = [(piece, piece)]
        for s in range(1, Z):
            step = [None, None]
            for kind, moves in edges(Z, s):
                step[kind] = send(got[s - 1][1 - kind], moves=moves)
            got.append(tuple(step))
        return got

    def source(z, kind, s):
        for a, b in dict(edges(Z, s)).get(kind, []):
            if b == z:
                return z - s if a < b else z + s
        return None

    def body(x_late, x_early, cotangent, pre_gain, post_gain, gate_weight, up_weight, down_weight, down_grad_sum):
        r, f, t = (lax.axis_index(a) for a in AXES)
        y, z = f % G, f // G
        n, D = x_late.shape
        m = n // T
        K, F = gate_weight.shape
        w = F // (R * G)
        PT = len(peers)

        def columns(weight, dy):
            q = r * G + (y + dy) % G
            return lax.dynamic_slice_in_dim(weight, q * w, w, 1)

        def both(dy):
            return jnp.concatenate([columns(gate_weight, dy), columns(up_weight, dy)], axis=1)

        gu = [both(0)] + [send(both(d), dy=d) for d in range(1, G)]
        dn = [columns(down_weight, 0)] + [send(columns(down_weight, d), dy=d) for d in range(1, G)]

        x = after(jnp.stack([x_late, x_early]), gu[0]).astype(f32)
        scale = lax.rsqrt(jnp.mean(x * x, axis=-1, keepdims=True) + eps)
        normed = (x * scale * pre_gain).astype(bf16).reshape(2, T, m, D)

        def chunk(array, j):
            return lax.dynamic_index_in_dim(array, (t + j) % T, 1, keepdims=False)

        def plane(value):
            out = []
            for p, (dr, dy) in enumerate(peers):
                got = send(value, dr=-dr, dy=-dy) if p else value
                out.append(got)
            return out

        def cores(got):
            return [got] + [send(got, dt=-j) for j in range(1, T)]

        held = [[chunk(normed, j) for j in range(T)]]
        held += [cores(got) for p, got in enumerate(plane(chunk(normed, 0))) if p]
        tokens = jnp.stack([jnp.stack([h[j] for h in held], axis=1) for j in range(T)], axis=1)
        tokens = tokens.reshape(2 * PT * n, D)

        full = jnp.zeros((Z, G, K, 2 * w), bf16)

        def place(array, value, zi, yi):
            return lax.dynamic_update_slice(array, value[None, None], (zi, yi, 0, 0))

        lines = [line(piece) for piece in gu]

        def target(kind, s):
            where = z
            for i in range(Z):
                j = source(i, kind, s)
                if j is not None:
                    where = jnp.where(z == i, j, where)
            return where

        for s in range(1, Z):
            for d, got in enumerate(lines):
                for kind, _ in edges(Z, s):
                    full = place(full, got[s][kind], target(kind, s), (y - d) % G)
        for d, piece in enumerate(gu):
            full = place(full, piece, z, (y - d) % G)
        full = full.reshape(D, 2 * w)

        both_out = jnp.dot(tokens, full, preferred_element_type=f32)
        gate, up = both_out[:, :w], both_out[:, w:]
        hidden = (jax.nn.silu(gate) * up).astype(bf16)

        block = jnp.zeros((G, K, w), bf16)
        for d, piece in enumerate(dn):
            block = put(block, piece, (y - d) % G)
        block = block.reshape(G * K, w)
        if Z > 1:
            block = after(block, *[v for v in lines[-1][Z - 2] if v is not None])
        got = arrived = line(block)
        tables = [[(s, k) for s in range(1, Z) for k in (0, 1) if source(i, k, s) is not None] for i in range(Z)]
        slots, ids = [[(block, list(range(Z)))]], [z]
        for k in range(Z - 1):
            slot, where = [], z
            for s, kind in sorted({tables[i][k] for i in range(Z)}):
                owners = [i for i in range(Z) if tables[i][k] == (s, kind)]
                slot.append((got[s][kind], owners))
                for i in owners:
                    where = jnp.where(z == i, source(i, kind, s), where)
            slots.append(slot)
            ids.append(where)
        z_ref = z.reshape(1)

        def plane_sum(low):
            total = low[0].astype(f32)
            for p, (dr, dy) in enumerate(peers):
                if p:
                    total = total + send(low[p], dr=dr, dy=dy).astype(f32)
            return total

        def reduce_plane(left, weight):
            got = []
            for j in range(1, T):
                value = nt(left[j], weight).astype(bf16)
                got.append(send(value, dt=j))
            chip = nt(left[0], weight)
            for value in got:
                chip = chip + value.astype(f32)
            low = chip.astype(bf16)
            low = low.reshape(PT, m, -1)
            return plane_sum([low[p] for p in range(PT)]), low

        by_core = hidden.reshape(2, T, PT * m, w)
        by_core = [by_core[:, j].reshape(2 * PT * m, w) for j in range(T)]
        groups = [[0, 1]] + [[k] for k in range(2, Z)] if Z > 1 else [[0]]
        totals, total_ids = [], []
        for group in groups:
            some = [slots[k] for k in group]
            got = []
            for j in range(1, T):
                value = sent_product(z_ref, by_core[j], some, Z)
                got.append(send(value, dt=j))
            low = chip_product(z_ref, by_core[0], got, some, Z, 2, PT)
            total = plane_sum(low)
            for i, k in enumerate(group):
                totals.append(total[:, i * G * K:(i + 1) * G * K])
                total_ids.append(ids[k])
        branch = arrange(totals, total_ids, Z)
        branch_l, branch_e = branch[:m], branch[m:]

        def own_rows(array):
            return lax.dynamic_slice_in_dim(array, t * m, m, 0)

        def all_rows(value):
            rows = [value] + [send(value, dt=-j) for j in range(1, T)]
            return arrange(rows, [(t + j) % T for j in range(T)], T, axis=0)

        early_rz = lax.rsqrt(jnp.mean(branch_e * branch_e, axis=-1, keepdims=True) + eps)
        cot_f = own_rows(cotangent).astype(f32)
        dpost = 0.5 * cot_f * post_gain
        dbranch = early_rz * (dpost - branch_e * early_rz * early_rz * jnp.mean(branch_e * dpost, axis=-1, keepdims=True))
        dbranch = dbranch.astype(bf16)

        late_rz = lax.rsqrt(jnp.mean(branch_l * branch_l, axis=-1, keepdims=True) + eps)
        y_late = (own_rows(x_late).astype(f32) + 0.5 * branch_l * late_rz * post_gain).astype(bf16)
        y_late = all_rows(y_late)

        down_full = jnp.zeros((Z, G * K, w), bf16)
        pieces, _ = lax.optimization_barrier(([[v for v, _ in slot] for slot in slots], dbranch))
        for slot, values, where in zip(slots, pieces, ids):
            value = values[0]
            for other, (_, owners) in zip(values[1:], slot[1:]):
                value = jnp.where(here(z, owners), other, value)
            down_full = put(down_full, value, where)
        down_full = down_full.reshape(D, w)
        raw = plane(dbranch)
        spread = [cores(h) for h in raw]
        spread = jnp.stack([jnp.stack([h[j] for h in spread]) for j in range(T)]).reshape(PT * n, D)
        dhidden = jnp.dot(spread, down_full, preferred_element_type=f32)
        gate_e, up_e = gate[PT * n:], up[PT * n:]
        sig = jax.nn.sigmoid(gate_e)
        dgate = (dhidden * up_e * sig * (1.0 + gate_e * (1.0 - sig))).astype(bf16)
        dup = (dhidden * gate_e * sig).astype(bf16)
        dgu = jnp.concatenate([dgate, dup], axis=1).reshape(T, PT * m, 2 * w)
        dnormed, dlow = reduce_plane([dgu[j] for j in range(T)], full)
        early_f = own_rows(x_early).astype(f32)
        early_rs = lax.dynamic_slice_in_dim(scale[1], t * m, m, 0)
        gained = pre_gain * dnormed
        dx = cot_f + early_rs * (gained - early_f * early_rs * early_rs * jnp.mean(early_f * gained, axis=-1, keepdims=True))
        dx = dx.astype(bf16)
        dx_early = all_rows(dx)

        hidden_e = hidden[PT * n:]
        if Z > 2:
            hidden_e = after(hidden_e, *[v for v in arrived[Z - 2] if v is not None])
        kept = [hidden_e] + [send(hidden_e, dz=k) for k in range(1, Z)]
        parts = after(dbranch, raw[ways[0]] if ways else dbranch).reshape(m, Z, G * K).transpose(1, 0, 2)
        cols = [pick(parts, z)] + [send(pick(parts, (z + k) % Z), dz=k) for k in range(1, Z)]
        wide = plane(after(jnp.stack(cols), *raw[1:]))
        wide = [cores(h) for h in wide]
        wide = [[wide[p][j] for p in range(PT)] for j in range(T)]
        wide, kept, _ = lax.optimization_barrier((wide, kept, dlow))
        wide = jnp.stack([jnp.stack(row) for row in wide])
        kept = jnp.stack([h.reshape(T, PT, m, w) for h in kept], axis=2)
        pieces, sources = [], []
        for a in range(R):
            grad = 0.0
            for j in range(T):
                left = wide[j, a * G:(a + 1) * G].reshape(G * Z * m, G * K)
                right = kept[j, a * G:(a + 1) * G].reshape(G * Z * m, w)
                grad = grad + tn(left, right)
            grad = grad.reshape(G, K, w)
            for b in range(G):
                piece = pick(grad, (y + b) % G)
                if a or b:
                    piece = send(piece.astype(bf16), dr=a, dy=b).astype(f32)
                pieces.append(piece)
                sources.append((r - a) % R * G + (y - b) % G)
        summed = arrange(pieces, sources, R * G)
        return (y_late, dx_early, down_grad_sum + summed)

    return body


def solution(mesh):
    R, S, T = (mesh.shape[a] for a in AXES)
    in_specs = (
        P(("rep", "fs"), None),
        P(("rep", "fs"), None),
        P(("rep", "fs"), None),
        P(),
        P(),
        P("fs", "tp"),
        P("fs", "tp"),
        P("fs", "tp"),
        P(("rep", "fs"), "tp"),
    )
    out_specs = (P(("rep", "fs"), None), P(("rep", "fs"), None), P(("rep", "fs"), "tp"))
    step = jax.shard_map(make_body(R, S, T), mesh=mesh, in_specs=in_specs, out_specs=out_specs, check_vma=False)
    if S // plan(R, S)[0] > 4:
        return step
    return step
```

```python
import jax
import jax.numpy as jnp
from jax import lax
from jax.experimental import pallas as pl
from jax.experimental.pallas import tpu as pltpu
from jax.sharding import PartitionSpec as P


eps = 1e-06
AXES = ("rep", "fs", "tp")
VMEM = 67_043_328
f32 = jnp.float32
bf16 = jnp.bfloat16


def nt(left, right):
    return lax.dot_general(left, right, (((1,), (1,)), ((), ())), preferred_element_type=f32)


def tn(left, right):
    return lax.dot_general(left, right, (((0,), (0,)), ((), ())), preferred_element_type=f32)


def put(array, value, index):
    return lax.dynamic_update_index_in_dim(array, value, index, 0)


def arrange(values, ids, count, axis=-1):
    out = []
    for i in range(count):
        value = values[0]
        for k in range(1, len(values)):
            value = jnp.where(ids[k] == i, values[k], value)
        out.append(value)
    return jnp.concatenate(out, axis=axis)


def after(value, *others):
    return lax.optimization_barrier((value,) + others)[0]


def whole(n, scalar=0):
    vmem = [pl.BlockSpec(memory_space=pltpu.VMEM)] * n
    return [pl.BlockSpec(memory_space=pltpu.SMEM)] * scalar + vmem


def here(z, owners):
    hit = z == owners[0]
    for i in owners[1:]:
        hit = hit | (z == i)
    return hit


def params(*arrays):
    held = sum(a.size * a.dtype.itemsize for a in arrays)
    return pltpu.CompilerParams(vmem_limit_bytes=max(2 * held, 1 << 20) + (2 << 20))


def cut(places, sources, shapes, jobs, room=None):
    lane = 128
    if any(job[2] % lane for job in jobs):
        outs = [jnp.zeros(shape, bf16) for shape in shapes]
        for src, place, width, out, row, col in jobs:
            block = lax.dynamic_slice_in_dim(sources[src], places[place] * width, width, 1)
            outs[out] = lax.dynamic_update_slice(outs[out], block, (row, col))
        return outs

    def kernel(place_ref, *refs):
        srcs, outs, sems = refs[:len(sources)], refs[len(sources):-1], refs[-1]
        copies = []
        for i, (src, place, width, out, row, col) in enumerate(jobs):
            start = pl.multiple_of(place_ref[place] * width, lane)
            rows = sources[src].shape[0]
            copies.append(pltpu.make_async_copy(
                srcs[src].at[:, pl.ds(start, width)], outs[out].at[row:row + rows, col:col + width], sems.at[i]))
        for copy in copies:
            copy.start()
        for copy in copies:
            copy.wait()

    outs = [jax.ShapeDtypeStruct(shape, bf16) for shape in shapes]
    return list(pl.pallas_call(
        kernel,
        out_shape=outs,
        in_specs=[pl.BlockSpec(memory_space=pltpu.SMEM)] + [pl.BlockSpec(memory_space=pl.ANY)] * len(sources),
        out_specs=whole(len(shapes)),
        scratch_shapes=[pltpu.SemaphoreType.DMA((len(jobs),))],
        compiler_params=params(*outs) if room is None else pltpu.CompilerParams(vmem_limit_bytes=VMEM - room),
        cost_estimate=pl.CostEstimate(flops=2_000_000, bytes_accessed=1 << 20, transcendentals=0),
    )(jnp.stack(places).astype(jnp.int32), *sources))


def by_slot(zref, slots, refs, count, emit):
    at = 0
    for k, slot in enumerate(slots):
        for owners in slot:
            ref = refs[at]
            at += 1
            if len(owners) == count:
                emit(k, ref)
            else:
                pl.when(here(zref[0], owners))(lambda k=k, ref=ref: emit(k, ref))


def sent_product(z, left, slots, count):
    rows, (columns, w) = left.shape[0], slots[0][0][0].shape
    owners = [[o for _, o in slot] for slot in slots]
    values = [v for slot in slots for v, _ in slot]

    def kernel(zref, left_ref, *refs):
        out = refs[-1]

        def emit(k, ref):
            out[:, k * columns:(k + 1) * columns] = nt(left_ref[...], ref[...]).astype(bf16)

        by_slot(zref, owners, refs, count, emit)

    return pl.pallas_call(
        kernel,
        out_shape=jax.ShapeDtypeStruct((rows, len(slots) * columns), bf16),
        in_specs=whole(1 + len(values), 1),
        out_specs=whole(1)[0],
        compiler_params=params(left, *values, left, left),
        cost_estimate=pl.CostEstimate(flops=2 * rows * w * columns * len(slots), bytes_accessed=4 * rows * columns, transcendentals=0),
    )(z, left, *values)


def chip_product(z, left, got, slots, count, lead, parts):
    rows, (columns, w) = left.shape[0], slots[0][0][0].shape
    m = rows // (lead * parts)
    owners = [[o for _, o in slot] for slot in slots]
    values = [v for slot in slots for v, _ in slot]

    def kernel(zref, left_ref, *refs):
        received, refs, outs = refs[:len(got)], refs[len(got):-parts], refs[-parts:]

        def emit(k, ref):
            span = slice(k * columns, (k + 1) * columns)
            chip = nt(left_ref[...], ref[...])
            for other in received:
                chip = chip + other[:, span].astype(f32)
            chip = chip.astype(bf16)
            for a in range(lead):
                for p, out in enumerate(outs):
                    out[a * m:(a + 1) * m, span] = chip[(a * parts + p) * m:(a * parts + p + 1) * m]

        by_slot(zref, owners, refs, count, emit)

    return pl.pallas_call(
        kernel,
        out_shape=[jax.ShapeDtypeStruct((lead * m, len(slots) * columns), bf16)] * parts,
        in_specs=whole(1 + len(got) + len(values), 1),
        out_specs=whole(parts),
        compiler_params=params(left, *values, *got, *got),
        cost_estimate=pl.CostEstimate(flops=2 * rows * w * columns * len(slots), bytes_accessed=8 * rows * columns, transcendentals=0),
    )(z, left, *got, *values)


def weight_gradient(places, left, right, cases, T, G):
    Z, (rows, high), wide = len(cases), left[0].shape, right[0].shape[1]
    K = high // G

    def kernel(place_ref, *refs):
        lefts, rights, outs, total = refs[:len(left)], refs[len(left):len(left) + len(right)], refs[-1 - G:-1], refs[-1]

        def case(i):
            value = None
            for index, k in cases[i]:
                a = jnp.concatenate([lefts[k * T + j][...] for j in range(T)], axis=0)
                term = tn(a, rights[index][...])
                value = term if value is None else value + term
            total[...] = value

        for i in range(Z):
            pl.when(place_ref[0] == i)(lambda i=i: case(i))
        for b, out in enumerate(outs):
            start = pl.multiple_of(lax.rem(place_ref[1] + b, G) * K, K)
            out[...] = total[pl.ds(start, K), :].astype(out.dtype)

    shapes = [jax.ShapeDtypeStruct((K, wide), bf16 if b else f32) for b in range(G)]
    scratch = jax.ShapeDtypeStruct((high, wide), f32)
    return pl.pallas_call(
        kernel,
        out_shape=shapes,
        in_specs=whole(len(left) + len(right), 1),
        out_specs=whole(G),
        scratch_shapes=[pltpu.VMEM((high, wide), f32)],
        compiler_params=params(*left, *right, *shapes, scratch, scratch),
        cost_estimate=pl.CostEstimate(flops=2 * Z * T * rows * high * wide, bytes_accessed=1 << 22, transcendentals=0),
    )(places.astype(jnp.int32), *left, *right)


def plan(R, S):
    G = 2 if S % 2 == 0 else 1
    Z = S // G
    peers = [(a, b) for a in range(R) for b in range(G)]
    ways = sorted(range(1, len(peers)), key=lambda p: (peers[p][0] != 0, peers[p][1] != 0))
    return G, Z, peers, ways


def edges(Z, s):
    out = []
    for kind in (0, 1):
        pairs = []
        for i in range(kind, Z - 1, 2):
            if i - (s - 1) >= 0:
                pairs.append((i, i + 1))
            if i + s < Z:
                pairs.append((i + 1, i))
        if pairs:
            out.append((kind, pairs))
    return out


def make_body(R, S, T):
    G, Z, peers, _ = plan(R, S)

    def send(value, dr=0, dy=0, dz=0, dt=0, moves=None):
        moves = [(z, (z + dz) % Z) for z in range(Z)] if moves is None else moves
        pairs = []
        for r in range(R):
            for z, to in moves:
                for y in range(G):
                    for t in range(T):
                        source = (r * S + z * G + y) * T + t
                        target = ((r + dr) % R * S + to * G + (y + dy) % G) * T + (t + dt) % T
                        pairs.append((source, target))
        return lax.ppermute(value, AXES, pairs)

    def line(piece):
        got = [(piece, piece)]
        for s in range(1, Z):
            step = [None, None]
            for kind, moves in edges(Z, s):
                step[kind] = send(got[s - 1][1 - kind], moves=moves)
            got.append(tuple(step))
        return got

    def partner(z, k):
        return z ^ k if Z & (Z - 1) == 0 else (z + k) % Z

    def source(z, kind, s):
        for a, b in dict(edges(Z, s)).get(kind, []):
            if b == z:
                return z - s if a < b else z + s
        return None

    def body(x_late, x_early, cotangent, pre_gain, post_gain, gate_weight, up_weight, down_weight, down_grad_sum):
        r, f, t = (lax.axis_index(a) for a in AXES)
        y, z = f % G, f // G
        n, D = x_late.shape
        m = n // T
        K, F = gate_weight.shape
        w = F // (R * G)
        PT = len(peers)

        def block(d):
            return r * G + (y + d) % G

        spots = [block(d) for d in range(G)]
        pairs = [(i, d, w, d, 0, i * w) for d in range(G) for i in range(2)]
        wide = cut(spots, [gate_weight, up_weight], [(K, 2 * w)] * G, pairs)
        thin = cut(spots, [down_weight], [(K, w)] * G, [(0, d, w, d, 0, 0) for d in range(G)])
        gu = wide[:1] + [send(wide[d], dy=d) for d in range(1, G)]
        dn = thin[:1] + [send(thin[d], dy=d) for d in range(1, G)]

        x = after(jnp.stack([x_late, x_early]), gu[0]).astype(f32)
        scale = lax.rsqrt(jnp.mean(x * x, axis=-1, keepdims=True) + eps)
        normed = (x * scale * pre_gain).astype(bf16).reshape(2, T, m, D)

        def chunk(array, j):
            return lax.dynamic_index_in_dim(array, (t + j) % T, 1, keepdims=False)

        def plane(value):
            out = []
            for p, (dr, dy) in enumerate(peers):
                got = send(value, dr=-dr, dy=-dy) if p else value
                out.append(got)
            return out

        def cores(got):
            return [got] + [send(got, dt=-j) for j in range(1, T)]

        held = [[chunk(normed, j) for j in range(T)]]
        held += [cores(got) for p, got in enumerate(plane(chunk(normed, 0))) if p]
        tokens = jnp.stack([jnp.stack([h[j] for h in held], axis=1) for j in range(T)], axis=1)
        tokens = tokens.reshape(2 * PT * n, D)

        full = jnp.zeros((Z, G, K, 2 * w), bf16)

        def place(array, value, zi, yi):
            return lax.dynamic_update_slice(array, value[None, None], (zi, yi, 0, 0))

        lines = [line(piece) for piece in gu]

        def target(kind, s):
            where = z
            for i in range(Z):
                j = source(i, kind, s)
                if j is not None:
                    where = jnp.where(z == i, j, where)
            return where

        for s in range(1, Z):
            for d, got in enumerate(lines):
                for kind, _ in edges(Z, s):
                    full = place(full, got[s][kind], target(kind, s), (y - d) % G)
        for d, piece in enumerate(gu):
            full = place(full, piece, z, (y - d) % G)
        full = full.reshape(D, 2 * w)

        halves = []
        for i in range(2):
            value = jnp.dot(tokens[i * PT * n:(i + 1) * PT * n], full, preferred_element_type=f32)
            gate, up = value[:, :w], value[:, w:]
            halves.append((jax.nn.silu(gate) * up).astype(bf16).reshape(T, PT * m, w))
        gate_e, up_e = gate, up

        block = arrange(dn, [(y - d) % G for d in range(G)], G, axis=0)
        if Z > 1:
            block = after(block, *[v for v in lines[-1][Z - 2] if v is not None])
        got = arrived = line(block)
        tables = [[(s, k) for s in range(1, Z) for k in (0, 1) if source(i, k, s) is not None] for i in range(Z)]
        slots, ids = [[(block, list(range(Z)))]], [z]
        for k in range(Z - 1):
            slot, where = [], z
            for s, kind in sorted({tables[i][k] for i in range(Z)}):
                owners = [i for i in range(Z) if tables[i][k] == (s, kind)]
                slot.append((got[s][kind], owners))
                for i in owners:
                    where = jnp.where(z == i, source(i, kind, s), where)
            slots.append(slot)
            ids.append(where)
        z_ref = z.reshape(1)

        def plane_sum(low):
            total = low[0].astype(f32)
            for p, (dr, dy) in enumerate(peers):
                if p:
                    total = total + send(low[p], dr=dr, dy=dy).astype(f32)
            return total

        def reduce_plane(left, weight):
            got = []
            for j in range(1, T):
                value = nt(left[j], weight).astype(bf16)
                got.append(send(value, dt=j))
            chip = nt(left[0], weight)
            for value in got:
                chip = chip + value.astype(f32)
            low = chip.astype(bf16)
            low = low.reshape(PT, m, -1)
            return plane_sum([low[p] for p in range(PT)]), low

        by_core = [jnp.concatenate([half[j] for half in halves]) for j in range(T)]
        groups = [[0, 1]] + [[k] for k in range(2, Z)] if Z > 1 else [[0]]
        totals, total_ids = [], []
        for group in groups:
            some = [slots[k] for k in group]
            got = []
            for j in range(1, T):
                value = sent_product(z_ref, by_core[j], some, Z)
                got.append(send(value, dt=j))
            low = chip_product(z_ref, by_core[0], got, some, Z, 2, PT)
            total = plane_sum(low)
            for i, k in enumerate(group):
                totals.append(total[:, i * G * K:(i + 1) * G * K])
                total_ids.append(ids[k])
        branch = arrange(totals, total_ids, Z)
        branch_l, branch_e = branch[:m], branch[m:]

        def own_rows(array):
            return lax.dynamic_slice_in_dim(array, t * m, m, 0)

        def all_rows(value):
            rows = [value] + [send(value, dt=-j) for j in range(1, T)]
            return arrange(rows, [(t + j) % T for j in range(T)], T, axis=0)

        early_rz = lax.rsqrt(jnp.mean(branch_e * branch_e, axis=-1, keepdims=True) + eps)
        cot_f = own_rows(cotangent).astype(f32)
        dpost = 0.5 * cot_f * post_gain
        dbranch = early_rz * (dpost - branch_e * early_rz * early_rz * jnp.mean(branch_e * dpost, axis=-1, keepdims=True))
        dbranch = dbranch.astype(bf16)

        late_rz = lax.rsqrt(jnp.mean(branch_l * branch_l, axis=-1, keepdims=True) + eps)
        y_late = (own_rows(x_late).astype(f32) + 0.5 * branch_l * late_rz * post_gain).astype(bf16)
        y_late = all_rows(y_late)

        down_full = jnp.zeros((Z, G * K, w), bf16)
        pieces, _ = lax.optimization_barrier(([[v for v, _ in slot] for slot in slots], dbranch))
        for slot, values, where in zip(slots, pieces, ids):
            value = values[0]
            for other, (_, owners) in zip(values[1:], slot[1:]):
                value = jnp.where(here(z, owners), other, value)
            down_full = put(down_full, value, where)
        down_full = down_full.reshape(D, w)
        raw = plane(dbranch)
        spread = spread_c = [cores(h) for h in raw]
        spread = jnp.stack([jnp.stack([h[j] for h in spread]) for j in range(T)]).reshape(PT * n, D)
        dhidden = jnp.dot(spread, down_full, preferred_element_type=f32)
        sig = jax.nn.sigmoid(gate_e)
        dgate = (dhidden * up_e * sig * (1.0 + gate_e * (1.0 - sig))).astype(bf16)
        dup = (dhidden * gate_e * sig).astype(bf16)
        dgu = jnp.concatenate([dgate, dup], axis=1).reshape(T, PT * m, 2 * w)
        dnormed, dlow = reduce_plane([dgu[j] for j in range(T)], full)
        early_f = own_rows(x_early).astype(f32)
        early_rs = lax.dynamic_slice_in_dim(scale[1], t * m, m, 0)
        gained = pre_gain * dnormed
        dx = cot_f + early_rs * (gained - early_f * early_rs * early_rs * jnp.mean(early_f * gained, axis=-1, keepdims=True))
        dx = dx.astype(bf16)
        dx_early = all_rows(dx)

        hidden_e = halves[1].reshape(T, R, G * m, w)
        units = [hidden_e[:, 0]] + [send(hidden_e[:, a], dr=a) for a in range(1, R)]
        units = jnp.concatenate([u.reshape(G * n, w) for u in units], axis=1)
        passed = line(units)
        own = [raw[b] for b in range(G)]
        cols = cut(
            [partner(z, k) for k in range(Z)], own, [(G * m, G * K)] * Z, [(b, k, G * K, k, b * m, 0) for k in range(Z) for b in range(G)])
        cols = [value if k == 0 else send(value, moves=[(i, partner(i, k)) for i in range(Z)]) for k, value in enumerate(cols)]
        mates = [[spread_c[b][j] for b in range(G)] for j in range(T)]
        left = []
        for k, value in enumerate(cols):
            left.append(value)
            for j in range(1, T):
                if k:
                    left.append(send(value, dt=-j))
                else:
                    left.extend(cut([z], mates[j], [(G * m, G * K)], [(b, 0, G * K, 0, b * m, 0) for b in range(G)]))
        right, cases = [units], [[(0, 0)] for _ in range(Z)]
        for s in range(1, Z):
            for kind, _ in edges(Z, s):
                for i in range(Z):
                    j = source(i, kind, s)
                    if j is not None:
                        cases[i].append((len(right), next(k for k in range(Z) if partner(j, k) == i)))
                right.append(passed[s][kind])
        left, right, _ = lax.optimization_barrier((left, right, dlow))
        grads = weight_gradient(jnp.stack([z, y]), left, right, cases, T, G)
        pieces, sources = [], []
        for b in range(G):
            piece = send(grads[b], dy=b).astype(f32) if b else grads[0]
            for a in range(R):
                pieces.append(piece[:, a * w:(a + 1) * w])
                sources.append((r - a) % R * G + (y - b) % G)
        summed = arrange(pieces, sources, R * G)
        return (y_late, dx_early, down_grad_sum + summed)

    return body


def solution(mesh):
    R, S, T = (mesh.shape[a] for a in AXES)
    in_specs = (
        P(("rep", "fs"), None),
        P(("rep", "fs"), None),
        P(("rep", "fs"), None),
        P(),
        P(),
        P("fs", "tp"),
        P("fs", "tp"),
        P("fs", "tp"),
        P(("rep", "fs"), "tp"),
    )
    out_specs = (P(("rep", "fs"), None), P(("rep", "fs"), None), P(("rep", "fs"), "tp"))
    step = jax.shard_map(make_body(R, S, T), mesh=mesh, in_specs=in_specs, out_specs=out_specs, check_vma=False)
    if S // plan(R, S)[0] > 4:
        return step
    return step
```

```python
import jax
import jax.numpy as jnp
from jax import lax
from jax.experimental import pallas as pl
from jax.experimental.pallas import tpu as pltpu
from jax.sharding import PartitionSpec as P


eps = 1e-06
AXES = ("rep", "fs", "tp")
VMEM = 67_043_328
f32 = jnp.float32
bf16 = jnp.bfloat16


def nt(left, right):
    return lax.dot_general(left, right, (((1,), (1,)), ((), ())), preferred_element_type=f32)


def tn(left, right):
    return lax.dot_general(left, right, (((0,), (0,)), ((), ())), preferred_element_type=f32)


def arrange(values, ids, count, axis=-1):
    out = []
    for i in range(count):
        value = values[0]
        for k in range(1, len(values)):
            value = jnp.where(ids[k] == i, values[k], value)
        out.append(value)
    return jnp.concatenate(out, axis=axis)


def after(value, *others):
    return lax.optimization_barrier((value,) + others)[0]


def whole(n, scalar=0):
    vmem = [pl.BlockSpec(memory_space=pltpu.VMEM)] * n
    return [pl.BlockSpec(memory_space=pltpu.SMEM)] * scalar + vmem


def here(z, owners):
    hit = z == owners[0]
    for i in owners[1:]:
        hit = hit | (z == i)
    return hit


def params(*arrays):
    held = sum(a.size * a.dtype.itemsize for a in arrays)
    return pltpu.CompilerParams(vmem_limit_bytes=max(2 * held, 1 << 20) + (2 << 20))


def cut(places, sources, shapes, jobs, room=None):
    lane = 128
    if any(job[2] % lane for job in jobs):
        outs = [jnp.zeros(shape, bf16) for shape in shapes]
        for src, place, width, out, row, col in jobs:
            block = lax.dynamic_slice_in_dim(sources[src], places[place] * width, width, 1)
            outs[out] = lax.dynamic_update_slice(outs[out], block, (row, col))
        return outs

    def kernel(place_ref, *refs):
        srcs, outs, sems = refs[:len(sources)], refs[len(sources):-1], refs[-1]
        copies = []
        for i, (src, place, width, out, row, col) in enumerate(jobs):
            start = pl.multiple_of(place_ref[place] * width, lane)
            rows = sources[src].shape[0]
            copies.append(pltpu.make_async_copy(
                srcs[src].at[:, pl.ds(start, width)], outs[out].at[row:row + rows, col:col + width], sems.at[i]))
        for copy in copies:
            copy.start()
        for copy in copies:
            copy.wait()

    outs = [jax.ShapeDtypeStruct(shape, bf16) for shape in shapes]
    return list(pl.pallas_call(
        kernel,
        out_shape=outs,
        in_specs=[pl.BlockSpec(memory_space=pltpu.SMEM)] + [pl.BlockSpec(memory_space=pl.ANY)] * len(sources),
        out_specs=whole(len(shapes)),
        scratch_shapes=[pltpu.SemaphoreType.DMA((len(jobs),))],
        compiler_params=params(*outs) if room is None else pltpu.CompilerParams(vmem_limit_bytes=VMEM - room),
        cost_estimate=pl.CostEstimate(flops=2_000_000, bytes_accessed=1 << 20, transcendentals=0),
    )(places, *sources))


def in_arrival(table, t, cotangent, gain, m, Z):
    D = gain.shape[1]
    B = D // Z

    def kernel(table_ref, core_ref, cot_ref, gain_ref, out_ref, post_ref):
        rows = pl.ds(pl.multiple_of(core_ref[0] * m, m), m)
        for k in range(Z):
            here_ = pl.ds(pl.multiple_of(table_ref[k] * B, B), B)
            there_ = slice(k * B, (k + 1) * B)
            scale = gain_ref[:, here_]
            post_ref[:, there_] = scale
            out_ref[:, there_] = 0.5 * cot_ref[rows, here_].astype(f32) * scale

    shapes = [jax.ShapeDtypeStruct((m, D), f32), jax.ShapeDtypeStruct((1, D), f32)]
    return pl.pallas_call(
        kernel,
        out_shape=shapes,
        in_specs=whole(2, 2),
        out_specs=whole(2),
        compiler_params=params(cotangent, gain, *shapes),
        cost_estimate=pl.CostEstimate(flops=4 * m * D, bytes_accessed=8 * m * D, transcendentals=0),
    )(table, t.reshape(1).astype(jnp.int32), cotangent, gain)


def by_slot(zref, slots, refs, count, emit):
    at = 0
    for k, slot in enumerate(slots):
        for owners in slot:
            ref = refs[at]
            at += 1
            if len(owners) == count:
                emit(k, ref)
            else:
                pl.when(here(zref[0], owners))(lambda k=k, ref=ref: emit(k, ref))


def sent_product(z, left, slots, count):
    rows, (columns, w) = left.shape[0], slots[0][0][0].shape
    owners = [[o for _, o in slot] for slot in slots]
    values = [v for slot in slots for v, _ in slot]

    def kernel(zref, left_ref, *refs):
        out = refs[-1]

        def emit(k, ref):
            out[:, k * columns:(k + 1) * columns] = nt(left_ref[...], ref[...]).astype(bf16)

        by_slot(zref, owners, refs, count, emit)

    return pl.pallas_call(
        kernel,
        out_shape=jax.ShapeDtypeStruct((rows, len(slots) * columns), bf16),
        in_specs=whole(1 + len(values), 1),
        out_specs=whole(1)[0],
        compiler_params=params(left, *values, left, left),
        cost_estimate=pl.CostEstimate(flops=2 * rows * w * columns * len(slots), bytes_accessed=4 * rows * columns, transcendentals=0),
    )(z, left, *values)


def chip_product(z, left, got, slots, count, lead, parts):
    rows, (columns, w) = left.shape[0], slots[0][0][0].shape
    m = rows // (lead * parts)
    owners = [[o for _, o in slot] for slot in slots]
    values = [v for slot in slots for v, _ in slot]

    def kernel(zref, left_ref, *refs):
        received, refs, outs = refs[:len(got)], refs[len(got):-parts], refs[-parts:]

        def emit(k, ref):
            span = slice(k * columns, (k + 1) * columns)
            chip = nt(left_ref[...], ref[...])
            for other in received:
                chip = chip + other[:, span].astype(f32)
            chip = chip.astype(bf16)
            for a in range(lead):
                for p, out in enumerate(outs):
                    out[a * m:(a + 1) * m, span] = chip[(a * parts + p) * m:(a * parts + p + 1) * m]

        by_slot(zref, owners, refs, count, emit)

    return pl.pallas_call(
        kernel,
        out_shape=[jax.ShapeDtypeStruct((lead * m, len(slots) * columns), bf16)] * parts,
        in_specs=whole(1 + len(got) + len(values), 1),
        out_specs=whole(parts),
        compiler_params=params(left, *values, *got, *got),
        cost_estimate=pl.CostEstimate(flops=2 * rows * w * columns * len(slots), bytes_accessed=8 * rows * columns, transcendentals=0),
    )(z, left, *got, *values)


def weight_gradient(places, left, right, cases, T, G):
    Z, (rows, high), wide = len(cases), left[0].shape, right[0].shape[1]
    K = high // G

    def kernel(place_ref, *refs):
        lefts, rights, outs, total = refs[:len(left)], refs[len(left):len(left) + len(right)], refs[-1 - G:-1], refs[-1]

        def case(i):
            value = None
            for index, k in cases[i]:
                a = jnp.concatenate([lefts[k * T + j][...] for j in range(T)], axis=0)
                term = tn(a, rights[index][...])
                value = term if value is None else value + term
            total[...] = value

        for i in range(Z):
            pl.when(place_ref[0] == i)(lambda i=i: case(i))
        for b, out in enumerate(outs):
            start = pl.multiple_of(lax.rem(place_ref[1] + b, G) * K, K)
            out[...] = total[pl.ds(start, K), :].astype(out.dtype)

    shapes = [jax.ShapeDtypeStruct((K, wide), bf16 if b else f32) for b in range(G)]
    scratch = jax.ShapeDtypeStruct((high, wide), f32)
    return pl.pallas_call(
        kernel,
        out_shape=shapes,
        in_specs=whole(len(left) + len(right), 1),
        out_specs=whole(G),
        scratch_shapes=[pltpu.VMEM((high, wide), f32)],
        compiler_params=params(*left, *right, *shapes, scratch, scratch),
        cost_estimate=pl.CostEstimate(flops=2 * Z * T * rows * high * wide, bytes_accessed=1 << 22, transcendentals=0),
    )(places.astype(jnp.int32), *left, *right)


def plan(R, S):
    G = 2 if S % 2 == 0 else 1
    Z = S // G
    peers = [(a, b) for a in range(R) for b in range(G)]
    ways = sorted(range(1, len(peers)), key=lambda p: (peers[p][0] != 0, peers[p][1] != 0))
    return G, Z, peers, ways


def edges(Z, s):
    out = []
    for kind in (0, 1):
        pairs = []
        for i in range(kind, Z - 1, 2):
            if i - (s - 1) >= 0:
                pairs.append((i, i + 1))
            if i + s < Z:
                pairs.append((i + 1, i))
        if pairs:
            out.append((kind, pairs))
    return out


def make_body(R, S, T):
    G, Z, peers, _ = plan(R, S)

    def send(value, dr=0, dy=0, dz=0, dt=0, moves=None):
        moves = [(z, (z + dz) % Z) for z in range(Z)] if moves is None else moves
        pairs = []
        for r in range(R):
            for z, to in moves:
                for y in range(G):
                    for t in range(T):
                        source = (r * S + z * G + y) * T + t
                        target = ((r + dr) % R * S + to * G + (y + dy) % G) * T + (t + dt) % T
                        pairs.append((source, target))
        return lax.ppermute(value, AXES, pairs)

    def line(piece):
        got = [(piece, piece)]
        for s in range(1, Z):
            step = [None, None]
            for kind, moves in edges(Z, s):
                step[kind] = send(got[s - 1][1 - kind], moves=moves)
            got.append(tuple(step))
        return got

    def partner(z, k):
        return z ^ k if Z & (Z - 1) == 0 else (z + k) % Z

    def source(z, kind, s):
        for a, b in dict(edges(Z, s)).get(kind, []):
            if b == z:
                return z - s if a < b else z + s
        return None

    def body(x_late, x_early, cotangent, pre_gain, post_gain, gate_weight, up_weight, down_weight, down_grad_sum):
        r, f, t = (lax.axis_index(a) for a in AXES)
        y, z = f % G, f // G
        n, D = x_late.shape
        m = n // T
        K, F = gate_weight.shape
        w = F // (R * G)
        PT = len(peers)

        def block(d):
            return r * G + (y + d) % G

        spots = jnp.stack([block(d) for d in range(G)]).astype(jnp.int32)
        pairs = [(i, d, w, d, 0, i * w) for d in range(G) for i in range(2)]
        wide = cut(spots, [gate_weight, up_weight], [(K, 2 * w)] * G, pairs)
        thin = cut(spots, [down_weight], [(K, w)] * G, [(0, d, w, d, 0, 0) for d in range(G)])
        gu = wide[:1] + [send(wide[d], dy=d) for d in range(1, G)]
        dn = thin[:1] + [send(thin[d], dy=d) for d in range(1, G)]

        x = after(jnp.stack([x_late, x_early]), gu[0]).astype(f32)
        scale = lax.rsqrt(jnp.mean(x * x, axis=-1, keepdims=True) + eps)
        normed = (x * scale * pre_gain).astype(bf16).reshape(2, T, m, D)

        def chunk(array, j):
            return lax.dynamic_index_in_dim(array, (t + j) % T, 1, keepdims=False)

        def plane(value):
            out = []
            for p, (dr, dy) in enumerate(peers):
                got = send(value, dr=-dr, dy=-dy) if p else value
                out.append(got)
            return out

        def cores(got):
            return [got] + [send(got, dt=-j) for j in range(1, T)]

        held = [[chunk(normed, j) for j in range(T)]]
        held += [cores(got) for p, got in enumerate(plane(chunk(normed, 0))) if p]
        tokens = jnp.stack([jnp.stack([h[j] for h in held], axis=1) for j in range(T)], axis=1)
        tokens = tokens.reshape(2 * PT * n, D)

        turn = [[i] + [source(i, k, s) for s in range(1, Z) for k in (0, 1) if source(i, k, s) is not None] for i in range(Z)]
        rows = [t_ + [t_.index(partner(i, k)) for k in range(Z)] + [0] for i, t_ in enumerate(turn)]
        table = lax.dynamic_slice_in_dim(jnp.asarray(rows, jnp.int32), z, 1, 0).reshape(-1)

        def own_rows(array):
            return lax.dynamic_slice_in_dim(array, t * m, m, 0)

        full = jnp.zeros((Z, G, K, 2 * w), bf16)

        def place(array, value, zi, yi):
            return lax.dynamic_update_slice(array, value[None, None], (zi, yi, 0, 0))

        lines = [line(piece) for piece in gu]

        def target(kind, s):
            where = z
            for i in range(Z):
                j = source(i, kind, s)
                if j is not None:
                    where = jnp.where(z == i, j, where)
            return where

        final = []
        for s in range(1, Z):
            for d, got in enumerate(lines):
                for kind, _ in edges(Z, s):
                    if (s, d) == (Z - 1, G - 1):
                        final.append((kind, got[s][kind]))
                        continue
                    full = place(full, got[s][kind], target(kind, s), (y - d) % G)
        for d, piece in enumerate(gu):
            full = place(full, piece, z, (y - d) % G)
        most, full_last = full.reshape(D, 2 * w), full
        ready = [v for v in lines[-1][max(Z - 2, 0)] if v is not None]
        cot_late, gain_late = lax.optimization_barrier((cotangent, post_gain, ready))[:2]
        dpost, post = in_arrival(table, t, cot_late, gain_late.reshape(1, D), m, Z)
        most, dpost, post = lax.optimization_barrier((most, dpost, post))
        y_last = (y - (G - 1)) % G
        lasts = []
        for kind, piece in final:
            at = (target(kind, Z - 1) * G + y_last) * K
            lasts.append((piece, lax.dynamic_slice_in_dim(tokens, at, K, 1)))

        def complete(*ready):
            out = full_last
            for kind, piece in final:
                piece, out = lax.optimization_barrier((piece, out) + ready)[:2]
                spot = target(kind, Z - 1)
                zs, ys = lax.broadcasted_iota(jnp.int32, (Z, G, 1, 1), 0), lax.broadcasted_iota(jnp.int32, (Z, G, 1, 1), 1)
                out = jnp.where((zs == spot) & (ys == y_last) & (spot != z), piece[None, None], out)
            return out.reshape(D, 2 * w)

        halves = []
        for i in range(2):
            rows = slice(i * PT * n, (i + 1) * PT * n)
            value = jnp.dot(tokens[rows], most, preferred_element_type=f32)
            value = after(value, *[p for line_ in lines[:-1] for p in line_[Z - 1] if p is not None])
            for piece, left in lasts:
                value = value + jnp.dot(left[rows], piece, preferred_element_type=f32)
            gate, up = value[:, :w], value[:, w:]
            sig = jax.nn.sigmoid(gate)
            halves.append((gate * sig * up).astype(bf16).reshape(T, PT * m, w))
        for_gate = (up * sig * (1.0 + gate * (1.0 - sig))).astype(bf16)
        for_up = (gate * sig).astype(bf16)
        for_gate, for_up = lax.optimization_barrier((for_gate, for_up))

        block = arrange(dn, [(y - d) % G for d in range(G)], G, axis=0)
        if Z > 1:
            block = after(block, *[v for v in lines[-1][Z - 2] if v is not None])
        got = arrived = line(block)
        tables = [[(s, k) for s in range(1, Z) for k in (0, 1) if source(i, k, s) is not None] for i in range(Z)]
        slots, ids = [[(block, list(range(Z)))]], [z]
        for k in range(Z - 1):
            slot, where = [], z
            for s, kind in sorted({tables[i][k] for i in range(Z)}):
                owners = [i for i in range(Z) if tables[i][k] == (s, kind)]
                slot.append((got[s][kind], owners))
                for i in owners:
                    where = jnp.where(z == i, source(i, kind, s), where)
            slots.append(slot)
            ids.append(where)
        z_ref = z.reshape(1)

        def plane_sum(low):
            total = low[0].astype(f32)
            for p, (dr, dy) in enumerate(peers):
                if p:
                    total = total + send(low[p], dr=dr, dy=dy).astype(f32)
            return total

        def reduce_plane(left, weight):
            got = []
            for j in range(1, T):
                value = nt(left[j], weight).astype(bf16)
                got.append(send(value, dt=j))
            chip = nt(left[0], weight)
            for value in got:
                chip = chip + value.astype(f32)
            low = chip.astype(bf16)
            low = low.reshape(PT, m, -1)
            return plane_sum([low[p] for p in range(PT)]), low

        by_core = [jnp.concatenate([half[j] for half in halves]) for j in range(T)]
        groups = [[0, 1]] + [[k] for k in range(2, Z)] if Z > 1 else [[0]]
        totals, total_ids = [], []
        for group in groups:
            some = [slots[k] for k in group]
            got = []
            for j in range(1, T):
                value = sent_product(z_ref, by_core[j], some, Z)
                got.append(send(value, dt=j))
            low = chip_product(z_ref, by_core[0], got, some, Z, 2, PT)
            totals.append(plane_sum(low))
            total_ids += [ids[k] for k in group]
        branch = jnp.concatenate(totals, axis=-1)
        branch_l, branch_e = branch[:m], branch[m:]

        def all_rows(value):
            rows = [value] + [send(value, dt=-j) for j in range(1, T)]
            return arrange(rows, [(t + j) % T for j in range(T)], T, axis=0)

        early_rz = lax.rsqrt(jnp.mean(branch_e * branch_e, axis=-1, keepdims=True) + eps)
        cot_f = own_rows(cotangent).astype(f32)
        dbranch = early_rz * (dpost - branch_e * early_rz * early_rz * jnp.mean(branch_e * dpost, axis=-1, keepdims=True))
        dbranch = dbranch.astype(bf16)

        late_rz = lax.rsqrt(jnp.mean(branch_l * branch_l, axis=-1, keepdims=True) + eps)
        added = 0.5 * branch_l * late_rz * post
        added = arrange([added[:, k * G * K:(k + 1) * G * K] for k in range(Z)], total_ids, Z)
        y_late = (own_rows(x_late).astype(f32) + added).astype(bf16)
        y_late = all_rows(y_late)

        pieces, _ = lax.optimization_barrier(([[v for v, _ in slot] for slot in slots], dbranch))
        down_full = []
        for slot, values in zip(slots, pieces):
            value = values[0]
            for other, (_, owners) in zip(values[1:], slot[1:]):
                value = jnp.where(here(z, owners), other, value)
            down_full.append(value)
        down_full = jnp.concatenate(down_full, axis=0)
        raw = plane(dbranch)
        spread = spread_c = [cores(h) for h in raw]
        spread = jnp.stack([jnp.stack([h[j] for h in spread]) for j in range(T)]).reshape(PT * n, D)
        dhidden = jnp.dot(spread, down_full, preferred_element_type=f32)
        dgate = (dhidden * for_gate.astype(f32)).astype(bf16)
        dup = (dhidden * for_up.astype(f32)).astype(bf16)
        dgu = jnp.concatenate([dgate, dup], axis=1).reshape(T, PT * m, 2 * w)
        full = complete(dbranch)
        dnormed, dlow = reduce_plane([dgu[j] for j in range(T)], full)
        early_f = own_rows(x_early).astype(f32)
        early_rs = lax.dynamic_slice_in_dim(scale[1], t * m, m, 0)
        gained = pre_gain * dnormed
        dx = cot_f + early_rs * (gained - early_f * early_rs * early_rs * jnp.mean(early_f * gained, axis=-1, keepdims=True))
        dx = dx.astype(bf16)
        dx_early = all_rows(dx)

        hidden_e = halves[1].reshape(T, R, G * m, w)
        units = [hidden_e[:, 0]] + [send(hidden_e[:, a], dr=a) for a in range(1, R)]
        units = jnp.concatenate([u.reshape(G * n, w) for u in units], axis=1)
        passed = line(units)
        own = [raw[b] for b in range(G)]
        cols = cut(
            table, own, [(G * m, G * K)] * Z, [(b, Z + k, G * K, k, b * m, 0) for k in range(Z) for b in range(G)])
        cols = [value if k == 0 else send(value, moves=[(i, partner(i, k)) for i in range(Z)]) for k, value in enumerate(cols)]
        mates = [[spread_c[b][j] for b in range(G)] for j in range(T)]
        left = []
        for k, value in enumerate(cols):
            left.append(value)
            for j in range(1, T):
                if k:
                    left.append(send(value, dt=-j))
                else:
                    left.extend(cut(table, mates[j], [(G * m, G * K)], [(b, Z, G * K, 0, b * m, 0) for b in range(G)]))
        right, cases = [units], [[(0, 0)] for _ in range(Z)]
        for s in range(1, Z):
            for kind, _ in edges(Z, s):
                for i in range(Z):
                    j = source(i, kind, s)
                    if j is not None:
                        cases[i].append((len(right), next(k for k in range(Z) if partner(j, k) == i)))
                right.append(passed[s][kind])
        left, right, _ = lax.optimization_barrier((left, right, dlow))
        grads = weight_gradient(jnp.stack([z, y]), left, right, cases, T, G)
        pieces, sources = [], []
        for b in range(G):
            piece = send(grads[b], dy=b) if b else grads[0]
            for a in range(R):
                pieces.append(piece[:, a * w:(a + 1) * w])
                sources.append((r - a) % R * G + (y - b) % G)
        mine, theirs = pieces[:R], pieces[R:]
        blank = [jnp.zeros((K, w), f32)] * (len(pieces) - R)
        partly = down_grad_sum + arrange(mine + blank, sources, R * G)
        if theirs:
            partly, theirs = lax.optimization_barrier((partly, theirs))
        total = partly + arrange([jnp.zeros((K, w), bf16)] * R + theirs, sources, R * G).astype(f32)
        return (y_late, dx_early, total)

    return body


def solution(mesh):
    R, S, T = (mesh.shape[a] for a in AXES)
    in_specs = (
        P(("rep", "fs"), None),
        P(("rep", "fs"), None),
        P(("rep", "fs"), None),
        P(),
        P(),
        P("fs", "tp"),
        P("fs", "tp"),
        P("fs", "tp"),
        P(("rep", "fs"), "tp"),
    )
    out_specs = (P(("rep", "fs"), None), P(("rep", "fs"), None), P(("rep", "fs"), "tp"))
    step = jax.shard_map(make_body(R, S, T), mesh=mesh, in_specs=in_specs, out_specs=out_specs, check_vma=False)
    if S // plan(R, S)[0] > 4:
        return step
    return step
```

```python
import jax
import jax.numpy as jnp
from jax import lax
from jax.experimental import pallas as pl
from jax.experimental.pallas import tpu as pltpu
from jax.sharding import PartitionSpec as P


eps = 1e-06
AXES = ("rep", "fs", "tp")
VMEM = 67_043_328
f32 = jnp.float32
bf16 = jnp.bfloat16


def nt(left, right):
    return lax.dot_general(left, right, (((1,), (1,)), ((), ())), preferred_element_type=f32)


def tn(left, right):
    return lax.dot_general(left, right, (((0,), (0,)), ((), ())), preferred_element_type=f32)


def arrange(values, ids, count, axis=-1):
    out = []
    for i in range(count):
        value = values[0]
        for k in range(1, len(values)):
            value = jnp.where(ids[k] == i, values[k], value)
        out.append(value)
    return jnp.concatenate(out, axis=axis)


def after(value, *others):
    return lax.optimization_barrier((value,) + others)[0]


def whole(n, scalar=0):
    vmem = [pl.BlockSpec(memory_space=pltpu.VMEM)] * n
    return [pl.BlockSpec(memory_space=pltpu.SMEM)] * scalar + vmem


def here(z, owners):
    hit = z == owners[0]
    for i in owners[1:]:
        hit = hit | (z == i)
    return hit


def params(*arrays):
    held = sum(a.size * a.dtype.itemsize for a in arrays)
    return pltpu.CompilerParams(vmem_limit_bytes=max(2 * held, 1 << 20) + (2 << 20))


def cut(places, sources, shapes, jobs, room=None):
    lane = 128
    if any(job[2] % lane for job in jobs):
        outs = [jnp.zeros(shape, bf16) for shape in shapes]
        for src, place, width, out, row, col in jobs:
            block = lax.dynamic_slice_in_dim(sources[src], places[place] * width, width, 1)
            outs[out] = lax.dynamic_update_slice(outs[out], block, (row, col))
        return outs

    def kernel(place_ref, *refs):
        srcs, outs, sems = refs[:len(sources)], refs[len(sources):-1], refs[-1]
        copies = []
        for i, (src, place, width, out, row, col) in enumerate(jobs):
            start = pl.multiple_of(place_ref[place] * width, lane)
            rows = sources[src].shape[0]
            copies.append(pltpu.make_async_copy(
                srcs[src].at[:, pl.ds(start, width)], outs[out].at[row:row + rows, col:col + width], sems.at[i]))
        for copy in copies:
            copy.start()
        for copy in copies:
            copy.wait()

    outs = [jax.ShapeDtypeStruct(shape, bf16) for shape in shapes]
    return list(pl.pallas_call(
        kernel,
        out_shape=outs,
        in_specs=[pl.BlockSpec(memory_space=pltpu.SMEM)] + [pl.BlockSpec(memory_space=pl.ANY)] * len(sources),
        out_specs=whole(len(shapes)),
        scratch_shapes=[pltpu.SemaphoreType.DMA((len(jobs),))],
        compiler_params=params(*outs) if room is None else pltpu.CompilerParams(vmem_limit_bytes=VMEM - room),
        cost_estimate=pl.CostEstimate(flops=2_000_000, bytes_accessed=1 << 20, transcendentals=0),
    )(places, *sources))


def in_arrival(table, t, cotangent, gain, m, Z):
    D = gain.shape[1]
    B = D // Z

    def kernel(table_ref, core_ref, cot_ref, gain_ref, out_ref, post_ref):
        rows = pl.ds(pl.multiple_of(core_ref[0] * m, m), m)
        for k in range(Z):
            here_ = pl.ds(pl.multiple_of(table_ref[k] * B, B), B)
            there_ = slice(k * B, (k + 1) * B)
            scale = gain_ref[:, here_]
            post_ref[:, there_] = scale
            out_ref[:, there_] = 0.5 * cot_ref[rows, here_].astype(f32) * scale

    shapes = [jax.ShapeDtypeStruct((m, D), f32), jax.ShapeDtypeStruct((1, D), f32)]
    return pl.pallas_call(
        kernel,
        out_shape=shapes,
        in_specs=whole(2, 2),
        out_specs=whole(2),
        compiler_params=params(cotangent, gain, *shapes),
        cost_estimate=pl.CostEstimate(flops=4 * m * D, bytes_accessed=8 * m * D, transcendentals=0),
    )(table, t.reshape(1).astype(jnp.int32), cotangent, gain)


def by_slot(zref, slots, refs, count, emit):
    at = 0
    for k, slot in enumerate(slots):
        for owners in slot:
            ref = refs[at]
            at += 1
            if len(owners) == count:
                emit(k, ref)
            else:
                pl.when(here(zref[0], owners))(lambda k=k, ref=ref: emit(k, ref))


def sent_product(z, left, slots, count):
    rows, (columns, w) = left.shape[0], slots[0][0][0].shape
    owners = [[o for _, o in slot] for slot in slots]
    values = [v for slot in slots for v, _ in slot]

    def kernel(zref, left_ref, *refs):
        out = refs[-1]

        def emit(k, ref):
            out[:, k * columns:(k + 1) * columns] = nt(left_ref[...], ref[...]).astype(bf16)

        by_slot(zref, owners, refs, count, emit)

    return pl.pallas_call(
        kernel,
        out_shape=jax.ShapeDtypeStruct((rows, len(slots) * columns), bf16),
        in_specs=whole(1 + len(values), 1),
        out_specs=whole(1)[0],
        compiler_params=params(left, *values, left, left),
        cost_estimate=pl.CostEstimate(flops=2 * rows * w * columns * len(slots), bytes_accessed=4 * rows * columns, transcendentals=0),
    )(z, left, *values)


def chip_product(z, left, got, slots, count, lead, parts):
    rows, (columns, w) = left.shape[0], slots[0][0][0].shape
    m = rows // (lead * parts)
    owners = [[o for _, o in slot] for slot in slots]
    values = [v for slot in slots for v, _ in slot]

    def kernel(zref, left_ref, *refs):
        received, refs, outs = refs[:len(got)], refs[len(got):-parts], refs[-parts:]

        def emit(k, ref):
            span = slice(k * columns, (k + 1) * columns)
            chip = nt(left_ref[...], ref[...])
            for other in received:
                chip = chip + other[:, span].astype(f32)
            chip = chip.astype(bf16)
            for a in range(lead):
                for p, out in enumerate(outs):
                    out[a * m:(a + 1) * m, span] = chip[(a * parts + p) * m:(a * parts + p + 1) * m]

        by_slot(zref, owners, refs, count, emit)

    return pl.pallas_call(
        kernel,
        out_shape=[jax.ShapeDtypeStruct((lead * m, len(slots) * columns), bf16)] * parts,
        in_specs=whole(1 + len(got) + len(values), 1),
        out_specs=whole(parts),
        compiler_params=params(left, *values, *got, *got),
        cost_estimate=pl.CostEstimate(flops=2 * rows * w * columns * len(slots), bytes_accessed=8 * rows * columns, transcendentals=0),
    )(z, left, *got, *values)


def weight_gradient(places, left, right, cases, T, G):
    Z, rows, high = left[0].shape
    wide, rows = right[0].shape[1], rows * G
    K = high // G

    def kernel(place_ref, *refs):
        lefts, rights, outs, total = refs[:len(left)], refs[len(left):len(left) + len(right)], refs[-1 - G:-1], refs[-1]

        def case(i):
            value = None
            for index, k in cases[i]:
                a = jnp.concatenate([ref[k] for ref in lefts], axis=0)
                term = tn(a, rights[index][...])
                value = term if value is None else value + term
            total[...] = value

        for i in range(Z):
            pl.when(place_ref[0] == i)(lambda i=i: case(i))
        for b, out in enumerate(outs):
            start = pl.multiple_of(lax.rem(place_ref[1] + b, G) * K, K)
            out[...] = total[pl.ds(start, K), :].astype(out.dtype)

    shapes = [jax.ShapeDtypeStruct((K, wide), bf16 if b else f32) for b in range(G)]
    scratch = jax.ShapeDtypeStruct((high, wide), f32)
    return pl.pallas_call(
        kernel,
        out_shape=shapes,
        in_specs=whole(len(left) + len(right), 1),
        out_specs=whole(G),
        scratch_shapes=[pltpu.VMEM((high, wide), f32)],
        compiler_params=params(*left, *right, *shapes, scratch, scratch),
        cost_estimate=pl.CostEstimate(flops=2 * Z * T * rows * high * wide, bytes_accessed=1 << 22, transcendentals=0),
    )(places.astype(jnp.int32), *left, *right)


def plan(R, S):
    G = 2 if S % 2 == 0 else 1
    Z = S // G
    peers = [(a, b) for a in range(R) for b in range(G)]
    ways = sorted(range(1, len(peers)), key=lambda p: (peers[p][0] != 0, peers[p][1] != 0))
    return G, Z, peers, ways


def edges(Z, s):
    out = []
    for kind in (0, 1):
        pairs = []
        for i in range(kind, Z - 1, 2):
            if i - (s - 1) >= 0:
                pairs.append((i, i + 1))
            if i + s < Z:
                pairs.append((i + 1, i))
        if pairs:
            out.append((kind, pairs))
    return out


def make_body(R, S, T):
    G, Z, peers, _ = plan(R, S)

    def send(value, dr=0, dy=0, dz=0, dt=0, moves=None):
        moves = [(z, (z + dz) % Z) for z in range(Z)] if moves is None else moves
        pairs = []
        for r in range(R):
            for z, to in moves:
                for y in range(G):
                    for t in range(T):
                        source = (r * S + z * G + y) * T + t
                        target = ((r + dr) % R * S + to * G + (y + dy) % G) * T + (t + dt) % T
                        pairs.append((source, target))
        return lax.ppermute(value, AXES, pairs)

    def line(piece):
        got = [(piece, piece)]
        for s in range(1, Z):
            step = [None, None]
            for kind, moves in edges(Z, s):
                step[kind] = send(got[s - 1][1 - kind], moves=moves)
            got.append(tuple(step))
        return got

    def partner(z, k):
        return z ^ k if Z & (Z - 1) == 0 else (z + k) % Z

    def source(z, kind, s):
        for a, b in dict(edges(Z, s)).get(kind, []):
            if b == z:
                return z - s if a < b else z + s
        return None

    def body(x_late, x_early, cotangent, pre_gain, post_gain, gate_weight, up_weight, down_weight, down_grad_sum):
        r, f, t = (lax.axis_index(a) for a in AXES)
        y, z = f % G, f // G
        n, D = x_late.shape
        m = n // T
        K, F = gate_weight.shape
        w = F // (R * G)
        PT = len(peers)

        def block(d):
            return r * G + (y + d) % G

        spots = jnp.stack([block(d) for d in range(G)]).astype(jnp.int32)
        pairs = [(i, d, w, d, 0, i * w) for d in range(G) for i in range(2)]
        wide = cut(spots, [gate_weight, up_weight], [(K, 2 * w)] * G, pairs)
        thin = cut(spots, [down_weight], [(K, w)] * G, [(0, d, w, d, 0, 0) for d in range(G)])
        gu = wide[:1] + [send(wide[d], dy=d) for d in range(1, G)]
        dn = thin[:1] + [send(thin[d], dy=d) for d in range(1, G)]

        x = after(jnp.stack([x_late, x_early]), gu[0]).astype(f32)
        scale = lax.rsqrt(jnp.mean(x * x, axis=-1, keepdims=True) + eps)
        normed = (x * scale * pre_gain).astype(bf16).reshape(2, T, m, D)

        def chunk(array, j):
            return lax.dynamic_index_in_dim(array, (t + j) % T, 1, keepdims=False)

        def plane(value):
            out = []
            for p, (dr, dy) in enumerate(peers):
                got = send(value, dr=-dr, dy=-dy) if p else value
                out.append(got)
            return out

        def cores(got):
            return [got] + [send(got, dt=-j) for j in range(1, T)]

        held = [[chunk(normed, j) for j in range(T)]]
        held += [cores(got) for p, got in enumerate(plane(chunk(normed, 0))) if p]
        tokens = jnp.stack([jnp.stack([h[j] for h in held], axis=1) for j in range(T)], axis=1)
        tokens = tokens.reshape(2 * PT * n, D)

        turn = [[i] + [source(i, k, s) for s in range(1, Z) for k in (0, 1) if source(i, k, s) is not None] for i in range(Z)]
        rows = [t_ + [t_.index(partner(i, k)) for k in range(Z)] + [0] for i, t_ in enumerate(turn)]
        table = lax.dynamic_slice_in_dim(jnp.asarray(rows, jnp.int32), z, 1, 0).reshape(-1)

        def own_rows(array):
            return lax.dynamic_slice_in_dim(array, t * m, m, 0)

        full = jnp.zeros((Z, G, K, 2 * w), bf16)

        def place(array, value, zi, yi):
            return lax.dynamic_update_slice(array, value[None, None], (zi, yi, 0, 0))

        lines = [line(piece) for piece in gu]

        def target(kind, s):
            where = z
            for i in range(Z):
                j = source(i, kind, s)
                if j is not None:
                    where = jnp.where(z == i, j, where)
            return where

        final = []
        for s in range(1, Z):
            for d, got in enumerate(lines):
                for kind, _ in edges(Z, s):
                    if (s, d) == (Z - 1, G - 1):
                        final.append((kind, got[s][kind]))
                        continue
                    full = place(full, got[s][kind], target(kind, s), (y - d) % G)
        for d, piece in enumerate(gu):
            full = place(full, piece, z, (y - d) % G)
        most, full_last = full.reshape(D, 2 * w), full
        ready = [v for v in lines[-1][max(Z - 2, 0)] if v is not None]
        cot_late, gain_late = lax.optimization_barrier((cotangent, post_gain, ready))[:2]
        dpost, post = in_arrival(table, t, cot_late, gain_late.reshape(1, D), m, Z)
        most, dpost, post = lax.optimization_barrier((most, dpost, post))
        y_last = (y - (G - 1)) % G
        lasts = []
        for kind, piece in final:
            at = (target(kind, Z - 1) * G + y_last) * K
            lasts.append((piece, lax.dynamic_slice_in_dim(tokens, at, K, 1)))

        def complete(*ready):
            out = full_last
            for kind, piece in final:
                piece, out = lax.optimization_barrier((piece, out) + ready)[:2]
                spot = target(kind, Z - 1)
                zs, ys = lax.broadcasted_iota(jnp.int32, (Z, G, 1, 1), 0), lax.broadcasted_iota(jnp.int32, (Z, G, 1, 1), 1)
                out = jnp.where((zs == spot) & (ys == y_last) & (spot != z), piece[None, None], out)
            return out.reshape(D, 2 * w)

        halves = []
        for i in range(2):
            rows = slice(i * PT * n, (i + 1) * PT * n)
            value = jnp.dot(tokens[rows], most, preferred_element_type=f32)
            value = after(value, *[p for line_ in lines[:-1] for p in line_[Z - 1] if p is not None])
            for piece, left in lasts:
                value = value + jnp.dot(left[rows], piece, preferred_element_type=f32)
            gate, up = value[:, :w], value[:, w:]
            sig = jax.nn.sigmoid(gate)
            halves.append((gate * sig * up).astype(bf16).reshape(T, PT * m, w))
        for_gate = (up * sig * (1.0 + gate * (1.0 - sig))).astype(bf16)
        for_up = (gate * sig).astype(bf16)
        for_gate, for_up = lax.optimization_barrier((for_gate, for_up))

        block = arrange(dn, [(y - d) % G for d in range(G)], G, axis=0)
        if Z > 1:
            block = after(block, *[v for v in lines[-1][Z - 2] if v is not None])
        got = arrived = line(block)
        tables = [[(s, k) for s in range(1, Z) for k in (0, 1) if source(i, k, s) is not None] for i in range(Z)]
        slots, ids = [[(block, list(range(Z)))]], [z]
        for k in range(Z - 1):
            slot, where = [], z
            for s, kind in sorted({tables[i][k] for i in range(Z)}):
                owners = [i for i in range(Z) if tables[i][k] == (s, kind)]
                slot.append((got[s][kind], owners))
                for i in owners:
                    where = jnp.where(z == i, source(i, kind, s), where)
            slots.append(slot)
            ids.append(where)
        z_ref = z.reshape(1)

        def plane_sum(low):
            total = low[0].astype(f32)
            for p, (dr, dy) in enumerate(peers):
                if p:
                    total = total + send(low[p], dr=dr, dy=dy).astype(f32)
            return total

        def reduce_plane(left, weight):
            got = []
            for j in range(1, T):
                value = nt(left[j], weight).astype(bf16)
                got.append(send(value, dt=j))
            chip = nt(left[0], weight)
            for value in got:
                chip = chip + value.astype(f32)
            low = chip.astype(bf16)
            low = low.reshape(PT, m, -1)
            return plane_sum([low[p] for p in range(PT)]), low

        by_core = [jnp.concatenate([half[j] for half in halves]) for j in range(T)]
        groups = [[0, 1]] + [[k] for k in range(2, Z)] if Z > 1 else [[0]]
        totals, total_ids = [], []
        for group in groups:
            some = [slots[k] for k in group]
            got = []
            for j in range(1, T):
                value = sent_product(z_ref, by_core[j], some, Z)
                got.append(send(value, dt=j))
            low = chip_product(z_ref, by_core[0], got, some, Z, 2, PT)
            totals.append(plane_sum(low))
            total_ids += [ids[k] for k in group]
        branch = jnp.concatenate(totals, axis=-1)
        branch_l, branch_e = branch[:m], branch[m:]

        def all_rows(value):
            rows = [value] + [send(value, dt=-j) for j in range(1, T)]
            return arrange(rows, [(t + j) % T for j in range(T)], T, axis=0)

        early_rz = lax.rsqrt(jnp.mean(branch_e * branch_e, axis=-1, keepdims=True) + eps)
        cot_f = own_rows(cotangent).astype(f32)
        dbranch = early_rz * (dpost - branch_e * early_rz * early_rz * jnp.mean(branch_e * dpost, axis=-1, keepdims=True))
        dbranch = dbranch.astype(bf16)

        late_rz = lax.rsqrt(jnp.mean(branch_l * branch_l, axis=-1, keepdims=True) + eps)
        added = 0.5 * branch_l * late_rz * post
        added = arrange([added[:, k * G * K:(k + 1) * G * K] for k in range(Z)], total_ids, Z)
        y_late = (own_rows(x_late).astype(f32) + added).astype(bf16)
        y_late = all_rows(y_late)

        pieces, _ = lax.optimization_barrier(([[v for v, _ in slot] for slot in slots], dbranch))
        down_full = []
        for slot, values in zip(slots, pieces):
            value = values[0]
            for other, (_, owners) in zip(values[1:], slot[1:]):
                value = jnp.where(here(z, owners), other, value)
            down_full.append(value)
        down_full = jnp.concatenate(down_full, axis=0)
        raw = plane(dbranch)
        spread = spread_c = [cores(h) for h in raw]
        spread = jnp.stack([jnp.stack([h[j] for h in spread]) for j in range(T)]).reshape(PT * n, D)
        dhidden = jnp.dot(spread, down_full, preferred_element_type=f32)
        dgate = (dhidden * for_gate.astype(f32)).astype(bf16)
        dup = (dhidden * for_up.astype(f32)).astype(bf16)
        dgu = jnp.concatenate([dgate, dup], axis=1).reshape(T, PT * m, 2 * w)
        full = complete(dbranch)
        dnormed, dlow = reduce_plane([dgu[j] for j in range(T)], full)
        early_f = own_rows(x_early).astype(f32)
        early_rs = lax.dynamic_slice_in_dim(scale[1], t * m, m, 0)
        gained = pre_gain * dnormed
        dx = cot_f + early_rs * (gained - early_f * early_rs * early_rs * jnp.mean(early_f * gained, axis=-1, keepdims=True))
        dx = dx.astype(bf16)
        dx_early = all_rows(dx)

        hidden_e = halves[1].reshape(T, R, G * m, w)
        units = [hidden_e[:, 0]] + [send(hidden_e[:, a], dr=a) for a in range(1, R)]
        units = jnp.concatenate([u.reshape(G * n, w) for u in units], axis=1)
        passed = line(units)
        cols = cut(table, [dbranch], [(m, G * K)] * Z, [(0, Z + k, G * K, k, 0, 0) for k in range(Z)])
        cols = [v if k == 0 else send(v, moves=[(i, partner(i, k)) for i in range(Z)]) for k, v in enumerate(cols)]
        cols = jnp.stack(cols)
        cols = [send(cols, dy=-b) if b else cols for b in range(G)]
        mates = [[send(v, dt=-j) for v in cols] for j in range(1, T)]
        left = cols + [v for row in mates for v in row]
        right, cases = [units], [[(0, 0)] for _ in range(Z)]
        for s in range(1, Z):
            for kind, _ in edges(Z, s):
                for i in range(Z):
                    j = source(i, kind, s)
                    if j is not None:
                        cases[i].append((len(right), next(k for k in range(Z) if partner(j, k) == i)))
                right.append(passed[s][kind])
        left, right, _ = lax.optimization_barrier((left, right, dlow))
        grads = weight_gradient(jnp.stack([z, y]), left, right, cases, T, G)
        pieces, sources = [], []
        for b in range(G):
            piece = send(grads[b], dy=b) if b else grads[0]
            for a in range(R):
                pieces.append(piece[:, a * w:(a + 1) * w])
                sources.append((r - a) % R * G + (y - b) % G)
        mine, theirs = pieces[:R], pieces[R:]
        blank = [jnp.zeros((K, w), f32)] * (len(pieces) - R)
        partly = down_grad_sum + arrange(mine + blank, sources, R * G)
        if theirs:
            partly, theirs = lax.optimization_barrier((partly, theirs))
        total = partly + arrange([jnp.zeros((K, w), bf16)] * R + theirs, sources, R * G).astype(f32)
        return (y_late, dx_early, total)

    return body


def solution(mesh):
    R, S, T = (mesh.shape[a] for a in AXES)
    in_specs = (
        P(("rep", "fs"), None),
        P(("rep", "fs"), None),
        P(("rep", "fs"), None),
        P(),
        P(),
        P("fs", "tp"),
        P("fs", "tp"),
        P("fs", "tp"),
        P(("rep", "fs"), "tp"),
    )
    out_specs = (P(("rep", "fs"), None), P(("rep", "fs"), None), P(("rep", "fs"), "tp"))
    step = jax.shard_map(make_body(R, S, T), mesh=mesh, in_specs=in_specs, out_specs=out_specs, check_vma=False)
    if S // plan(R, S)[0] > 4:
        return step
    return step
```

```python
import jax
import jax.numpy as jnp
from jax import lax
from jax.experimental import pallas as pl
from jax.experimental.pallas import tpu as pltpu
from jax.sharding import PartitionSpec as P


eps = 1e-06
AXES = ("rep", "fs", "tp")
VMEM = 67_043_328
f32 = jnp.float32
bf16 = jnp.bfloat16


def nt(left, right):
    return lax.dot_general(left, right, (((1,), (1,)), ((), ())), preferred_element_type=f32)


def tn(left, right):
    return lax.dot_general(left, right, (((0,), (0,)), ((), ())), preferred_element_type=f32)


def arrange(values, ids, count, axis=-1):
    out = []
    for i in range(count):
        value = values[0]
        for k in range(1, len(values)):
            value = jnp.where(ids[k] == i, values[k], value)
        out.append(value)
    return jnp.concatenate(out, axis=axis)


def after(value, *others):
    return lax.optimization_barrier((value,) + others)[0]


def whole(n, scalar=0):
    vmem = [pl.BlockSpec(memory_space=pltpu.VMEM)] * n
    return [pl.BlockSpec(memory_space=pltpu.SMEM)] * scalar + vmem


def here(z, owners):
    hit = z == owners[0]
    for i in owners[1:]:
        hit = hit | (z == i)
    return hit


def params(*arrays):
    held = sum(a.size * a.dtype.itemsize for a in arrays)
    return pltpu.CompilerParams(vmem_limit_bytes=max(2 * held, 1 << 20) + (2 << 20))


def cut(places, sources, shapes, jobs, room=None):
    lane = 128
    if any(job[2] % lane for job in jobs):
        outs = [jnp.zeros(shape, bf16) for shape in shapes]
        for src, place, width, out, row, col in jobs:
            block = lax.dynamic_slice_in_dim(sources[src], places[place] * width, width, 1)
            outs[out] = lax.dynamic_update_slice(outs[out], block, (row, col))
        return outs

    def kernel(place_ref, *refs):
        srcs, outs, sems = refs[:len(sources)], refs[len(sources):-1], refs[-1]
        copies = []
        for i, (src, place, width, out, row, col) in enumerate(jobs):
            start = pl.multiple_of(place_ref[place] * width, lane)
            rows = sources[src].shape[0]
            copies.append(pltpu.make_async_copy(
                srcs[src].at[:, pl.ds(start, width)], outs[out].at[row:row + rows, col:col + width], sems.at[i]))
        for copy in copies:
            copy.start()
        for copy in copies:
            copy.wait()

    outs = [jax.ShapeDtypeStruct(shape, bf16) for shape in shapes]
    return list(pl.pallas_call(
        kernel,
        out_shape=outs,
        in_specs=[pl.BlockSpec(memory_space=pltpu.SMEM)] + [pl.BlockSpec(memory_space=pl.ANY)] * len(sources),
        out_specs=whole(len(shapes)),
        scratch_shapes=[pltpu.SemaphoreType.DMA((len(jobs),))],
        compiler_params=params(*outs) if room is None else pltpu.CompilerParams(vmem_limit_bytes=VMEM - room),
        cost_estimate=pl.CostEstimate(flops=2_000_000, bytes_accessed=1 << 20, transcendentals=0),
    )(places, *sources))


def in_arrival(table, t, cotangent, gain, m, Z):
    D = gain.shape[1]
    B = D // Z

    def kernel(table_ref, core_ref, cot_ref, gain_ref, out_ref, post_ref):
        rows = pl.ds(pl.multiple_of(core_ref[0] * m, m), m)
        for k in range(Z):
            here_ = pl.ds(pl.multiple_of(table_ref[k] * B, B), B)
            there_ = slice(k * B, (k + 1) * B)
            scale = gain_ref[:, here_]
            post_ref[:, there_] = scale
            out_ref[:, there_] = 0.5 * cot_ref[rows, here_].astype(f32) * scale

    shapes = [jax.ShapeDtypeStruct((m, D), f32), jax.ShapeDtypeStruct((1, D), f32)]
    return pl.pallas_call(
        kernel,
        out_shape=shapes,
        in_specs=whole(2, 2),
        out_specs=whole(2),
        compiler_params=params(cotangent, gain, *shapes),
        cost_estimate=pl.CostEstimate(flops=4 * m * D, bytes_accessed=8 * m * D, transcendentals=0),
    )(table, t.reshape(1).astype(jnp.int32), cotangent, gain)


def by_slot(zref, slots, refs, count, emit):
    at = 0
    for k, slot in enumerate(slots):
        for owners in slot:
            ref = refs[at]
            at += 1
            if len(owners) == count:
                emit(k, ref)
            else:
                pl.when(here(zref[0], owners))(lambda k=k, ref=ref: emit(k, ref))


def sent_product(z, left, slots, count):
    rows, (columns, w) = left.shape[0], slots[0][0][0].shape
    owners = [[o for _, o in slot] for slot in slots]
    values = [v for slot in slots for v, _ in slot]

    def kernel(zref, left_ref, *refs):
        out = refs[-1]

        def emit(k, ref):
            out[:, k * columns:(k + 1) * columns] = nt(left_ref[...], ref[...]).astype(bf16)

        by_slot(zref, owners, refs, count, emit)

    return pl.pallas_call(
        kernel,
        out_shape=jax.ShapeDtypeStruct((rows, len(slots) * columns), bf16),
        in_specs=whole(1 + len(values), 1),
        out_specs=whole(1)[0],
        compiler_params=params(left, *values, left, left),
        cost_estimate=pl.CostEstimate(flops=2 * rows * w * columns * len(slots), bytes_accessed=4 * rows * columns, transcendentals=0),
    )(z, left, *values)


def chip_product(z, left, got, slots, count, lead, parts):
    rows, (columns, w) = left.shape[0], slots[0][0][0].shape
    m = rows // (lead * parts)
    owners = [[o for _, o in slot] for slot in slots]
    values = [v for slot in slots for v, _ in slot]

    def kernel(zref, left_ref, *refs):
        received, refs, outs = refs[:len(got)], refs[len(got):-parts], refs[-parts:]

        def emit(k, ref):
            span = slice(k * columns, (k + 1) * columns)
            chip = nt(left_ref[...], ref[...])
            for other in received:
                chip = chip + other[:, span].astype(f32)
            chip = chip.astype(bf16)
            for a in range(lead):
                for p, out in enumerate(outs):
                    out[a * m:(a + 1) * m, span] = chip[(a * parts + p) * m:(a * parts + p + 1) * m]

        by_slot(zref, owners, refs, count, emit)

    return pl.pallas_call(
        kernel,
        out_shape=[jax.ShapeDtypeStruct((lead * m, len(slots) * columns), bf16)] * parts,
        in_specs=whole(1 + len(got) + len(values), 1),
        out_specs=whole(parts),
        compiler_params=params(left, *values, *got, *got),
        cost_estimate=pl.CostEstimate(flops=2 * rows * w * columns * len(slots), bytes_accessed=8 * rows * columns, transcendentals=0),
    )(z, left, *got, *values)


def weight_gradient(places, left, right, cases, T, G):
    Z, rows, high = left[0].shape
    wide, rows = right[0].shape[1], rows * G
    K = high // G

    def kernel(place_ref, *refs):
        lefts, rights, outs, total = refs[:len(left)], refs[len(left):len(left) + len(right)], refs[-1 - G:-1], refs[-1]

        def case(i):
            value = None
            for index, k in cases[i]:
                a = jnp.concatenate([ref[k] for ref in lefts], axis=0)
                term = tn(a, rights[index][...])
                value = term if value is None else value + term
            total[...] = value

        for i in range(Z):
            pl.when(place_ref[0] == i)(lambda i=i: case(i))
        for b, out in enumerate(outs):
            start = pl.multiple_of(lax.rem(place_ref[1] + b, G) * K, K)
            out[...] = total[pl.ds(start, K), :].astype(out.dtype)

    shapes = [jax.ShapeDtypeStruct((K, wide), bf16 if b else f32) for b in range(G)]
    scratch = jax.ShapeDtypeStruct((high, wide), f32)
    return pl.pallas_call(
        kernel,
        out_shape=shapes,
        in_specs=whole(len(left) + len(right), 1),
        out_specs=whole(G),
        scratch_shapes=[pltpu.VMEM((high, wide), f32)],
        compiler_params=params(*left, *right, *shapes, scratch, scratch),
        cost_estimate=pl.CostEstimate(flops=2 * Z * T * rows * high * wide, bytes_accessed=1 << 22, transcendentals=0),
    )(places.astype(jnp.int32), *left, *right)


def plan(R, S):
    G = 2 if S % 2 == 0 else 1
    Z = S // G
    peers = [(a, b) for a in range(R) for b in range(G)]
    ways = sorted(range(1, len(peers)), key=lambda p: (peers[p][0] != 0, peers[p][1] != 0))
    return G, Z, peers, ways


def edges(Z, s):
    out = []
    for kind in (0, 1):
        pairs = []
        for i in range(kind, Z - 1, 2):
            if i - (s - 1) >= 0:
                pairs.append((i, i + 1))
            if i + s < Z:
                pairs.append((i + 1, i))
        if pairs:
            out.append((kind, pairs))
    return out


def make_body(R, S, T):
    G, Z, peers, _ = plan(R, S)

    def send(value, dr=0, dy=0, dz=0, dt=0, moves=None):
        moves = [(z, (z + dz) % Z) for z in range(Z)] if moves is None else moves
        pairs = []
        for r in range(R):
            for z, to in moves:
                for y in range(G):
                    for t in range(T):
                        source = (r * S + z * G + y) * T + t
                        target = ((r + dr) % R * S + to * G + (y + dy) % G) * T + (t + dt) % T
                        pairs.append((source, target))
        return lax.ppermute(value, AXES, pairs)

    def line(piece):
        got = [(piece, piece)]
        for s in range(1, Z):
            step = [None, None]
            for kind, moves in edges(Z, s):
                step[kind] = send(got[s - 1][1 - kind], moves=moves)
            got.append(tuple(step))
        return got

    def partner(z, k):
        return z ^ k if Z & (Z - 1) == 0 else (z + k) % Z

    def source(z, kind, s):
        for a, b in dict(edges(Z, s)).get(kind, []):
            if b == z:
                return z - s if a < b else z + s
        return None

    def body(x_late, x_early, cotangent, pre_gain, post_gain, gate_weight, up_weight, down_weight, down_grad_sum):
        r, f, t = (lax.axis_index(a) for a in AXES)
        y, z = f % G, f // G
        n, D = x_late.shape
        m = n // T
        K, F = gate_weight.shape
        w = F // (R * G)
        PT = len(peers)

        def block(d):
            return r * G + (y + d) % G

        spots = jnp.stack([block(d) for d in range(G)]).astype(jnp.int32)
        pairs = [(i, d, w, d, 0, i * w) for d in range(G) for i in range(2)]
        wide = cut(spots, [gate_weight, up_weight], [(K, 2 * w)] * G, pairs)
        thin = cut(spots, [down_weight], [(K, w)] * G, [(0, d, w, d, 0, 0) for d in range(G)])
        gu = wide[:1] + [send(wide[d], dy=d) for d in range(1, G)]
        dn = thin[:1] + [send(thin[d], dy=d) for d in range(1, G)]

        x = after(jnp.stack([x_late, x_early]), gu[0]).astype(f32)
        scale = lax.rsqrt(jnp.mean(x * x, axis=-1, keepdims=True) + eps)
        normed = (x * scale * pre_gain).astype(bf16).reshape(2, T, m, D)

        def chunk(array, j):
            return lax.dynamic_index_in_dim(array, (t + j) % T, 1, keepdims=False)

        def plane(value):
            out = []
            for p, (dr, dy) in enumerate(peers):
                got = send(value, dr=-dr, dy=-dy) if p else value
                out.append(got)
            return out

        def cores(got):
            return [got] + [send(got, dt=-j) for j in range(1, T)]

        held = [[chunk(normed, j) for j in range(T)]]
        held += [cores(got) for p, got in enumerate(plane(chunk(normed, 0))) if p]
        tokens = jnp.stack([jnp.stack([h[j] for h in held], axis=1) for j in range(T)], axis=1)
        tokens = tokens.reshape(2 * PT * n, D)

        turn = [[i] + [source(i, k, s) for s in range(1, Z) for k in (0, 1) if source(i, k, s) is not None] for i in range(Z)]
        rows = [t_ + [t_.index(partner(i, k)) for k in range(Z)] + [0] for i, t_ in enumerate(turn)]
        table = lax.dynamic_slice_in_dim(jnp.asarray(rows, jnp.int32), z, 1, 0).reshape(-1)

        def own_rows(array):
            return lax.dynamic_slice_in_dim(array, t * m, m, 0)

        full = jnp.zeros((Z, G, K, 2 * w), bf16)

        def place(array, value, zi, yi):
            return lax.dynamic_update_slice(array, value[None, None], (zi, yi, 0, 0))

        lines = [line(piece) for piece in gu]

        def target(kind, s):
            where = z
            for i in range(Z):
                j = source(i, kind, s)
                if j is not None:
                    where = jnp.where(z == i, j, where)
            return where

        final = []
        for s in range(1, Z):
            for d, got in enumerate(lines):
                for kind, _ in edges(Z, s):
                    if (s, d) == (Z - 1, G - 1):
                        final.append((kind, got[s][kind]))
                        continue
                    full = place(full, got[s][kind], target(kind, s), (y - d) % G)
        for d, piece in enumerate(gu):
            full = place(full, piece, z, (y - d) % G)
        most, full_last = full.reshape(D, 2 * w), full
        ready = [v for v in lines[-1][max(Z - 2, 0)] if v is not None]
        cot_late, gain_late = lax.optimization_barrier((cotangent, post_gain, ready))[:2]
        dpost, post = in_arrival(table, t, cot_late, gain_late.reshape(1, D), m, Z)
        most, dpost, post = lax.optimization_barrier((most, dpost, post))
        y_last = (y - (G - 1)) % G
        lasts = []
        for kind, piece in final:
            at = (target(kind, Z - 1) * G + y_last) * K
            lasts.append((piece, lax.dynamic_slice_in_dim(tokens, at, K, 1)))

        def complete(*ready):
            out = full_last
            for kind, piece in final:
                piece, out = lax.optimization_barrier((piece, out) + ready)[:2]
                spot = target(kind, Z - 1)
                zs, ys = lax.broadcasted_iota(jnp.int32, (Z, G, 1, 1), 0), lax.broadcasted_iota(jnp.int32, (Z, G, 1, 1), 1)
                out = jnp.where((zs == spot) & (ys == y_last) & (spot != z), piece[None, None], out)
            return out.reshape(D, 2 * w)

        halves = []
        for i in range(2):
            rows = slice(i * PT * n, (i + 1) * PT * n)
            value = jnp.dot(tokens[rows], most, preferred_element_type=f32)
            value = after(value, *[p for line_ in lines[:-1] for p in line_[Z - 1] if p is not None])
            for piece, left in lasts:
                value = value + jnp.dot(left[rows], piece, preferred_element_type=f32)
            gate, up = value[:, :w], value[:, w:]
            sig = jax.nn.sigmoid(gate)
            halves.append((gate * sig * up).astype(bf16).reshape(T, PT * m, w))
        for_gate = (up * sig * (1.0 + gate * (1.0 - sig))).astype(bf16)
        for_up = (gate * sig).astype(bf16)
        by_rep = [[v.reshape(T, R, G * m, w)[:, a].reshape(G * n, w) for v in (for_gate, for_up)] for a in range(R)]
        by_rep = lax.optimization_barrier(by_rep)

        block = arrange(dn, [(y - d) % G for d in range(G)], G, axis=0)
        if Z > 1:
            block = after(block, *[v for v in lines[-1][Z - 2] if v is not None])
        got = arrived = line(block)
        tables = [[(s, k) for s in range(1, Z) for k in (0, 1) if source(i, k, s) is not None] for i in range(Z)]
        slots, ids = [[(block, list(range(Z)))]], [z]
        for k in range(Z - 1):
            slot, where = [], z
            for s, kind in sorted({tables[i][k] for i in range(Z)}):
                owners = [i for i in range(Z) if tables[i][k] == (s, kind)]
                slot.append((got[s][kind], owners))
                for i in owners:
                    where = jnp.where(z == i, source(i, kind, s), where)
            slots.append(slot)
            ids.append(where)
        z_ref = z.reshape(1)

        def plane_sum(low):
            total = low[0].astype(f32)
            for p, (dr, dy) in enumerate(peers):
                if p:
                    total = total + send(low[p], dr=dr, dy=dy).astype(f32)
            return total

        by_core = [jnp.concatenate([half[j] for half in halves]) for j in range(T)]
        groups = [[0, 1]] + [[k] for k in range(2, Z)] if Z > 1 else [[0]]
        totals, total_ids = [], []
        for group in groups:
            some = [slots[k] for k in group]
            got = []
            for j in range(1, T):
                value = sent_product(z_ref, by_core[j], some, Z)
                got.append(send(value, dt=j))
            low = chip_product(z_ref, by_core[0], got, some, Z, 2, PT)
            totals.append(plane_sum(low))
            total_ids += [ids[k] for k in group]
        branch = jnp.concatenate(totals, axis=-1)
        branch_l, branch_e = branch[:m], branch[m:]

        def all_rows(value):
            rows = [value] + [send(value, dt=-j) for j in range(1, T)]
            return arrange(rows, [(t + j) % T for j in range(T)], T, axis=0)

        early_rz = lax.rsqrt(jnp.mean(branch_e * branch_e, axis=-1, keepdims=True) + eps)
        cot_f = own_rows(cotangent).astype(f32)
        dbranch = early_rz * (dpost - branch_e * early_rz * early_rz * jnp.mean(branch_e * dpost, axis=-1, keepdims=True))
        dbranch = dbranch.astype(bf16)

        late_rz = lax.rsqrt(jnp.mean(branch_l * branch_l, axis=-1, keepdims=True) + eps)
        added = 0.5 * branch_l * late_rz * post
        added = arrange([added[:, k * G * K:(k + 1) * G * K] for k in range(Z)], total_ids, Z)
        y_late = (own_rows(x_late).astype(f32) + added).astype(bf16)
        y_late = all_rows(y_late)

        pieces, _ = lax.optimization_barrier(([[v for v, _ in slot] for slot in slots], dbranch))
        down_full = []
        for slot, values in zip(slots, pieces):
            value = values[0]
            for other, (_, owners) in zip(values[1:], slot[1:]):
                value = jnp.where(here(z, owners), other, value)
            down_full.append(value)
        down_full = jnp.concatenate(down_full, axis=0)
        raw = plane(dbranch)
        spread = [cores(h) for h in raw]
        full = complete(dbranch)
        dnormed = None
        for a in range(R):
            some = range(a * G, (a + 1) * G)
            rows = jnp.stack([jnp.stack([spread[p][j] for p in some]) for j in range(T)]).reshape(G * n, D)
            dhidden = jnp.dot(rows, down_full, preferred_element_type=f32)
            dgu = jnp.concatenate([(dhidden * v.astype(f32)).astype(bf16) for v in by_rep[a]], axis=1)
            dgu = dgu.reshape(T, G * m, 2 * w)
            got = []
            for j in range(1, T):
                value = nt(dgu[j], full).astype(bf16)
                got.append(send(value, dt=j))
            chip = nt(dgu[0], full)
            for value in got:
                chip = chip + value.astype(f32)
            dlow = chip.astype(bf16).reshape(G, m, D)
            for b in range(G):
                p = a * G + b
                term = (send(dlow[b], dr=a, dy=b) if p else dlow[b]).astype(f32)
                dnormed = term if dnormed is None else dnormed + term
        early_f = own_rows(x_early).astype(f32)
        early_rs = lax.dynamic_slice_in_dim(scale[1], t * m, m, 0)
        gained = pre_gain * dnormed
        dx = cot_f + early_rs * (gained - early_f * early_rs * early_rs * jnp.mean(early_f * gained, axis=-1, keepdims=True))
        dx = dx.astype(bf16)
        dx_early = all_rows(dx)

        hidden_e = halves[1].reshape(T, R, G * m, w)
        units = [hidden_e[:, 0]] + [send(hidden_e[:, a], dr=a) for a in range(1, R)]
        units = jnp.concatenate([u.reshape(G * n, w) for u in units], axis=1)
        passed = line(units)
        cols = cut(table, [dbranch], [(m, G * K)] * Z, [(0, Z + k, G * K, k, 0, 0) for k in range(Z)])
        cols = [v if k == 0 else send(v, moves=[(i, partner(i, k)) for i in range(Z)]) for k, v in enumerate(cols)]
        cols = jnp.stack(cols)
        cols = [send(cols, dy=-b) if b else cols for b in range(G)]
        mates = [[send(v, dt=-j) for v in cols] for j in range(1, T)]
        left = cols + [v for row in mates for v in row]
        right, cases = [units], [[(0, 0)] for _ in range(Z)]
        for s in range(1, Z):
            for kind, _ in edges(Z, s):
                for i in range(Z):
                    j = source(i, kind, s)
                    if j is not None:
                        cases[i].append((len(right), next(k for k in range(Z) if partner(j, k) == i)))
                right.append(passed[s][kind])
        left, right, _ = lax.optimization_barrier((left, right, dlow))
        grads = weight_gradient(jnp.stack([z, y]), left, right, cases, T, G)
        pieces, sources = [], []
        for b in range(G):
            piece = send(grads[b], dy=b) if b else grads[0]
            for a in range(R):
                pieces.append(piece[:, a * w:(a + 1) * w])
                sources.append((r - a) % R * G + (y - b) % G)
        mine, theirs = pieces[:R], pieces[R:]
        blank = [jnp.zeros((K, w), f32)] * (len(pieces) - R)
        partly = down_grad_sum + arrange(mine + blank, sources, R * G)
        if theirs:
            partly, theirs = lax.optimization_barrier((partly, theirs))
        total = partly + arrange([jnp.zeros((K, w), bf16)] * R + theirs, sources, R * G).astype(f32)
        return (y_late, dx_early, total)

    return body


def solution(mesh):
    R, S, T = (mesh.shape[a] for a in AXES)
    in_specs = (
        P(("rep", "fs"), None),
        P(("rep", "fs"), None),
        P(("rep", "fs"), None),
        P(),
        P(),
        P("fs", "tp"),
        P("fs", "tp"),
        P("fs", "tp"),
        P(("rep", "fs"), "tp"),
    )
    out_specs = (P(("rep", "fs"), None), P(("rep", "fs"), None), P(("rep", "fs"), "tp"))
    step = jax.shard_map(make_body(R, S, T), mesh=mesh, in_specs=in_specs, out_specs=out_specs, check_vma=False)
    if S // plan(R, S)[0] > 4:
        return step
    return step
```
